256 devices in a mesh: sp: 64 (over z, y, core), tp: 4 (over x).
Axes of the slice: x: 4, y: 4, z: 8, core: 2. Of those that a mesh axis runs over, the one named last changes fastest.
Arguments:
- residual: bfloat16 [12288, 2048], P(('sp', 'tp')), may hold values from -6 to 6
- mixer_input: bfloat16 [12288, 512], P('sp', 'tp'), may hold values from -6 to 6
- log_gate: float32 [12288, 32], P('sp', 'tp'), may hold values from -2 to 0
- decay_rate: float32 [2, 32, 64], P(None, 'tp'), may hold values from 0 to 1
- turn_rate: float32 [2, 32, 64], P(None, 'tp'), may hold values from -1 to 1
- drive_real: float32 [2, 32, 16, 64], P(None, 'tp'), may hold values from -1 to 1
- drive_imaginary: float32 [2, 32, 16, 64], P(None, 'tp'), may hold values from -1 to 1
- read_real: float32 [2, 32, 16, 64], P(None, 'tp'), may hold values from -0.75 to 0.75
- read_imaginary: float32 [2, 32, 16, 64], P(None, 'tp'), may hold values from -0.75 to 0.75
- skip_gain: float32 [512], P('tp'), may hold values from -4 to 4
- project_weight: bfloat16 [512, 2048], replicated, may hold values from -0.25 to 0.25
- norm_gain: float32 [2048], replicated, may hold values from 0.1 to 1.9
- final_gain: float32 [2048], replicated, may hold values from 0.1 to 1.9
- routes: int32 [12288, 2], P('sp'), may hold values from 0 to 63, all different within a row; in each aligned block of 48 rows (0 to 47, 48 to 95, ...) at most 2 rows name the same one
- group_weight: float32 [12288], P('sp'), may hold values from 0.2 to 1
- expert_weight: float32 [12288, 2], P('sp'), may hold values from 0.1 to 1
- gate_weight: bfloat16 [64, 2048, 1024], P('sp', None, 'tp'), may hold values from -0.125 to 0.125
- linear_weight: bfloat16 [64, 2048, 1024], P('sp', None, 'tp'), may hold values from -0.125 to 0.125
- down_weight: bfloat16 [64, 1024, 2048], P('sp', 'tp'), may hold values from -0.1875 to 0.1875
Outputs:
- finished: bfloat16 [12288, 2048], P(('sp', 'tp'))
The draws below stay inside these ranges and needn't reach their ends.
Inputs may be any that keep to these rules, and one draw needn't show every extreme that they name: `routes`: each row names 2 different experts. In each aligned block of 48 rows no expert is named by more than 2 rows; some expert is named by exactly 2 rows of some block.
All inputs are finite; a program needn't handle non-finite values.
Results may differ from the reference program's by a relative error of at most 0.006.
Values may be sent and summed in bfloat16 or wider, within the bound.
A program may use at most 128 MiB of HBM per device.

```python
import math
import jax
import jax.numpy as jnp
import numpy as np
from jax import lax

D = 2048
S_GROUPS = 32
GROUP_DIM = 16
S_STATE = 64
S_WIDTH = 512
D_EXPERT = 1024
TOP_K = 2
TOK_DEV = 192
TOKENS = 12288
TOK_SHARE = 48
EXPERTS = 64
SLOTS = 2
N_SP = 64
N_TP = 4


def draw_decay_rate(key, part):
    pick_key, fast_key, slow_key = jax.random.split(key, 3)
    fast_share = 0.5
    is_fast = jax.random.uniform(pick_key, (2, S_GROUPS, 1)) < fast_share
    fast_rate = jnp.exp(jax.random.uniform(fast_key, (2, S_GROUPS, S_STATE), minval=jnp.log(0.01), maxval=jnp.log(1.0 / 30.0)))
    slow_rate = jnp.exp(jax.random.uniform(slow_key, (2, S_GROUPS, S_STATE), minval=jnp.log(0.05), maxval=jnp.log(0.3))) / TOKENS
    return jnp.where(is_fast, fast_rate, slow_rate).astype(jnp.float32)


def draw_log_gate(key, part):
    factor_key, rough_key, place_key, drop_key = jax.random.split(key, 4)
    blocks = TOKENS // TOK_DEV
    factor = jnp.exp(jax.random.uniform(factor_key, (blocks, 1, S_GROUPS), minval=0.0, maxval=jnp.log(4.0)))
    roughness = jnp.exp(0.5 * jnp.clip(jax.random.normal(rough_key, (blocks, TOK_DEV, S_GROUPS)), -3.0, 3.0))
    steady = -0.2 / TOKENS * (factor * roughness).reshape(TOKENS, S_GROUPS)
    places = jax.random.randint(place_key, (2,), 0, TOKENS)
    drop_sizes = jnp.log(jax.random.uniform(drop_key, (2, S_GROUPS), minval=0.5, maxval=0.8))
    matches = (jnp.arange(TOKENS, dtype=jnp.int32)[:, None] == places[None, :]).astype(jnp.float32)
    return (steady + jnp.dot(matches, drop_sizes, precision=lax.Precision.HIGHEST)).astype(jnp.float32)


def shard_levels(stream_key, shape, pieces, smallest, high):
    def one(axis_at, shards_of):
        draws = jax.random.uniform(jax.random.fold_in(jax.random.fold_in(stream_key, 6), axis_at), (shards_of,), jnp.float32, smallest / len(pieces), high / len(pieces))
        return jnp.repeat(jnp.exp(draws), shape[axis_at] // shards_of).reshape((-1,) + (1,) * (len(shape) - axis_at - 1))

    level = one(*pieces[0])
    for cut in pieces[1:]:
        level = level * one(*cut)
    return level


def assign_block(rng, own, number, rows, number_of, top, most, skew):
    ranking = jax.random.permutation(rng, number_of)
    heavy_load, common = shares(number_of, rows * top, most, skew, True), shares(number_of, rows * top, most, skew, False)
    places = jnp.arange(number_of)

    def named(tallies, turn):
        used = int((tallies > 0).sum())
        fixed = max(1, used // 4)
        passed = fixed + (places - fixed + turn * (used - fixed)) % max(1, number_of - fixed)
        return jnp.zeros((number_of,), jnp.int32).at[ranking[jnp.where(places < fixed, places, passed)]].set(jnp.asarray(tallies, jnp.int32))

    tallies = jnp.where(number % 4 == 0, named(heavy_load, number // 4), named(common, number - number // 4 - 1))
    mixed = jax.random.permutation(jax.random.fold_in(own, 3), number_of)
    source_of, taker = mixed[0:number_of // 2 * 2:2], mixed[1:number_of // 2 * 2:2]
    room = jnp.minimum(tallies[source_of] - 1, most - tallies[taker]) // 2
    room = jnp.where((source_of == ranking[0]) | (taker == ranking[0]) | (tallies[taker] == 0), 0, jnp.maximum(room, 0))
    passed = jax.random.randint(jax.random.fold_in(own, 4), (number_of // 2,), 0, 1 << 20) % (room + 1)
    tallies = tallies.at[source_of].add(-passed).at[taker].add(passed)
    labels = jnp.searchsorted(jnp.cumsum(tallies), jnp.arange(rows * top), side="right").astype(jnp.int32)
    table = labels.reshape(top, rows).T
    table = table[jax.random.permutation(jax.random.fold_in(own, 1), rows)]
    turn = jax.random.randint(jax.random.fold_in(own, 2), (rows, 1), 0, top)
    return jnp.take_along_axis(table, (jnp.arange(top)[None, :] + turn) % top, axis=1)


def shares(count, total, limit, slope, full):
    weights = [(1 << 20) // math.isqrt(grade ** slope) + 1 for grade in range(1, count + 1)]
    largest = limit if full else min(limit, max(-(-total // count), total * weights[0] // sum(weights)))
    least = 1 if total - largest >= count - 1 else 0
    given, surplus = [largest] + [least] * (count - 1), total - largest - least * (count - 1)
    while surplus > 0:
        candidates = [i for i in range(1, count) if given[i] < largest] or [i for i in range(1, count) if given[i] < limit]
        pool, budget = sum([weights[i] for i in candidates]), surplus
        for i in candidates:
            extra = min(limit - given[i], max(1, budget * weights[i] // pool), surplus)
            given[i] = given[i] + extra
            surplus = surplus - extra
    return np.array(given)


def centred(key, extent, width, most, cuts=(), kind=jnp.bfloat16):
    drawn = width * jax.random.normal(key, extent, jnp.float32)
    if cuts:
        drawn = drawn * shard_levels(key, extent, cuts, -0.22, 0.18)
    return jnp.clip(drawn, -most, most).astype(kind)


def setup_inputs(seed: int = 0) -> dict:
    key_list = jax.random.split(jax.random.key(seed), 20)
    residual = centred(key_list[0], (TOKENS, D), 1.0, 6.0, ((0, 256),))
    mixer_input = centred(key_list[1], (TOKENS, S_WIDTH), 1.0, 6.0, ((0, 64), (1, 4)))
    log_gate = draw_log_gate(jax.random.fold_in(key_list[19], 71), 0)
    decay_rate = draw_decay_rate(jax.random.fold_in(key_list[19], 71), 0)
    turn_rate = jnp.clip(jax.random.uniform(key_list[4], (2, S_GROUPS, S_STATE), jnp.float32, -1.0, 1.0) * shard_levels(key_list[4], (2, S_GROUPS, S_STATE), ((1, 4),), -0.4, 0.0), -1.0, 1.0)
    drive_real = centred(key_list[5], (2, S_GROUPS, GROUP_DIM, S_STATE), (2 * GROUP_DIM) ** -0.5, 1.0, ((1, 4),), jnp.float32)
    drive_imaginary = centred(key_list[6], (2, S_GROUPS, GROUP_DIM, S_STATE), (2 * GROUP_DIM) ** -0.5, 1.0, ((1, 4),), jnp.float32)
    read_real = centred(key_list[7], (2, S_GROUPS, GROUP_DIM, S_STATE), S_STATE ** -0.5, 0.75, ((1, 4),), jnp.float32)
    read_imaginary = centred(key_list[8], (2, S_GROUPS, GROUP_DIM, S_STATE), S_STATE ** -0.5, 0.75, ((1, 4),), jnp.float32)
    skip_gain = centred(key_list[9], (S_WIDTH,), 1.0, 4.0, ((0, 4),), jnp.float32)
    project_weight = centred(key_list[10], (S_WIDTH, D), S_WIDTH ** -0.5, 0.25)
    norm_gain = jnp.clip(1.0 + 0.18 * jax.random.normal(key_list[11], (D,), jnp.float32), 0.1, 1.9)
    final_gain = jnp.clip(1.0 + 0.18 * jax.random.normal(key_list[12], (D,), jnp.float32), 0.1, 1.9)
    routes_keys = jax.random.split(jax.random.fold_in(key_list[13], 1), TOKENS // TOK_SHARE)
    routes_turns = jax.random.permutation(jax.random.fold_in(key_list[13], 3), TOKENS // TOK_SHARE)
    routes = jax.vmap(lambda own, number: assign_block(jax.random.fold_in(key_list[13], 2), own, number, TOK_SHARE, EXPERTS, TOP_K, SLOTS, 2))(routes_keys, routes_turns).reshape((TOKENS, TOP_K))
    group_weight = jnp.clip(jnp.exp(math.log(1.0) - 1.609438 * jax.random.uniform(key_list[14], (TOKENS,), jnp.float32) ** shard_levels(key_list[14], (TOKENS,), ((0, 64),), -0.2, 0.2)), 0.2, 1.0)
    expert_weight = jnp.clip(jnp.exp(math.log(1.0) - 2.3025851 * jax.random.uniform(key_list[15], (TOKENS, TOP_K), jnp.float32) ** shard_levels(key_list[15], (TOKENS, TOP_K), ((0, 64),), -0.2, 0.2)), 0.1, 1.0)
    gate_weight = centred(key_list[16], (EXPERTS, D, D_EXPERT), D ** -0.5, 0.125, ((0, 64), (2, 4)))
    linear_weight = centred(key_list[17], (EXPERTS, D, D_EXPERT), D ** -0.5, 0.125, ((0, 64), (2, 4)))
    down_weight = centred(key_list[18], (EXPERTS, D_EXPERT, D), D_EXPERT ** -0.5, 0.1875, ((0, 64), (1, 4)))
    return {"residual": residual, "mixer_input": mixer_input, "log_gate": log_gate, "decay_rate": decay_rate, "turn_rate": turn_rate, "drive_real": drive_real, "drive_imaginary": drive_imaginary, "read_real": read_real, "read_imaginary": read_imaginary, "skip_gain": skip_gain, "project_weight": project_weight, "norm_gain": norm_gain, "final_gain": final_gain, "routes": routes, "group_weight": group_weight, "expert_weight": expert_weight, "gate_weight": gate_weight, "linear_weight": linear_weight, "down_weight": down_weight}


deep_alpha = 2.0 ** 0.25
norm_epsilon = 1e-05
highest = lax.Precision.HIGHEST

def layer_norm(values, gain):
    center = values - lax.optimization_barrier(jnp.mean(values, axis=-1, keepdims=True))
    spread = lax.optimization_barrier(jnp.mean(center * center, axis=-1, keepdims=True))
    return center * lax.rsqrt(spread + norm_epsilon) * gain

def sweep(inputs, log_gate, rate_row, turn_row, drive_real, drive_imaginary, read_real, read_imaginary, backward):
    input_scale = jnp.sqrt(1.0 - jnp.exp(-2.0 * rate_row))
    retain = jnp.exp(-rate_row)
    step_real = retain * jnp.cos(turn_row)
    step_imaginary = retain * jnp.sin(turn_row)

    def advance(carried, current):
        state_real, state_imaginary = carried
        token_row, gate_row = current
        push_real = jnp.einsum('gh,ghp->gp', token_row, drive_real, precision=highest) * input_scale
        push_imaginary = jnp.einsum('gh,ghp->gp', token_row, drive_imaginary, precision=highest) * input_scale
        factor = jnp.exp(gate_row)[:, None]
        new_real = factor * (step_real * state_real - step_imaginary * state_imaginary) + push_real
        new_imaginary = factor * (step_real * state_imaginary + step_imaginary * state_real) + push_imaginary
        output = jnp.einsum('gp,ghp->gh', new_real, read_real, precision=highest) - jnp.einsum('gp,ghp->gh', new_imaginary, read_imaginary, precision=highest)
        return ((new_real, new_imaginary), output)
    initial = jnp.zeros(rate_row.shape, jnp.float32)
    _, outputs = lax.scan(advance, (initial, initial), (inputs, log_gate), reverse=backward)
    return outputs

def reference(residual, mixer_input, log_gate, decay_rate, turn_rate, drive_real, drive_imaginary, read_real, read_imaginary, skip_gain, project_weight, norm_gain, final_gain, routes, group_weight, expert_weight, gate_weight, linear_weight, down_weight):
    inputs = mixer_input.astype(jnp.float32).reshape(TOKENS, S_GROUPS, GROUP_DIM)
    readout = sweep(inputs, log_gate, decay_rate[0], turn_rate[0], drive_real[0], drive_imaginary[0], read_real[0], read_imaginary[0], False)
    readout = readout + sweep(inputs, log_gate, decay_rate[1], turn_rate[1], drive_real[1], drive_imaginary[1], read_real[1], read_imaginary[1], True)
    readout = readout + skip_gain.reshape(S_GROUPS, GROUP_DIM) * inputs
    activated = jax.nn.gelu(readout).reshape(TOKENS, S_WIDTH).astype(jnp.bfloat16)
    branch = jnp.dot(activated, project_weight, preferred_element_type=jnp.float32)
    middle = layer_norm(deep_alpha * residual.astype(jnp.float32) + branch, norm_gain)
    middle_rows = middle.astype(jnp.bfloat16)
    flat_experts = routes.reshape(-1)
    sorted_order = jnp.argsort(flat_experts, stable=True).astype(jnp.int32)
    counts = lax.optimization_barrier(jnp.sum((flat_experts[:, None] == jnp.arange(EXPERTS, dtype=jnp.int32)[None, :]).astype(jnp.int32), axis=0))
    starts = (jnp.cumsum(counts) - counts).astype(jnp.int32)
    capacity = N_SP * N_TP * SLOTS
    assigned = TOKENS * TOP_K
    piece_width = D_EXPERT // N_TP

    def run_expert(expert):
        offsets = jnp.arange(capacity, dtype=jnp.int32)
        is_valid = offsets < counts[expert]
        chosen = sorted_order[jnp.minimum(starts[expert] + offsets, assigned - 1)]
        row_inputs = middle_rows[chosen // TOP_K]
        gate_part = jnp.dot(row_inputs, gate_weight[expert], preferred_element_type=jnp.float32)
        linear_part = jnp.dot(row_inputs, linear_weight[expert], preferred_element_type=jnp.float32)
        hidden = (jax.nn.silu(gate_part) * linear_part).astype(jnp.bfloat16)
        running = jnp.zeros((capacity, D), jnp.float32)
        for member in range(N_TP):
            partial_value = jnp.dot(hidden[:, member * piece_width:(member + 1) * piece_width], down_weight[expert, member * piece_width:(member + 1) * piece_width], preferred_element_type=jnp.float32)
            rounded = lax.optimization_barrier(partial_value.astype(jnp.bfloat16))
            running = running + rounded.astype(jnp.float32)
        return (running.astype(jnp.bfloat16), jnp.where(is_valid, chosen, assigned).astype(jnp.int32))
    results, targets = lax.map(run_expert, jnp.arange(EXPERTS, dtype=jnp.int32))
    answers = jnp.zeros((assigned, D), jnp.bfloat16).at[targets.reshape(-1)].set(results.reshape(-1, D), mode='drop')
    mixing = group_weight[:, None] * expert_weight / lax.optimization_barrier(jnp.sum(expert_weight, axis=1, keepdims=True))
    routed = lax.optimization_barrier(jnp.sum(mixing[:, :, None] * answers.reshape(TOKENS, TOP_K, D).astype(jnp.float32), axis=1))
    finished = layer_norm(deep_alpha * middle + routed, final_gain)
    return finished.astype(jnp.bfloat16)
```

```python
import jax
import jax.numpy as jnp
from jax import lax
from jax.experimental import pallas as pl
from jax.experimental.pallas import tpu as pltpu
from jax.sharding import PartitionSpec as P

MESH = pl.DeviceIdType.MESH
F32 = jnp.float32
BF16 = jnp.bfloat16
deep_alpha = 2.0**0.25
norm_epsilon = 1e-05
SEGMENT = 24
CHUNKS = 4
WIDE = 512


def iota(shape, dim):
    return lax.broadcasted_iota(jnp.int32, shape, dim)


def cmul(a, b):
    return (a[0] * b[0] - a[1] * b[1], a[0] * b[1] + a[1] * b[0])


def dot(a, b):
    return jnp.dot(a, b, preferred_element_type=F32)


def dot_nt(a, b):
    return lax.dot_general(a, b, (((1,), (1,)), ((), ())), preferred_element_type=F32)


def dot_tn(a, b):
    return lax.dot_general(a, b, (((0,), (0,)), ((), ())), preferred_element_type=F32)


def halves(value):
    high = value.astype(BF16)
    return high, (value - high.astype(F32)).astype(BF16)


def one_minus_exp_neg(x):
    series = x * (1.0 - x * (0.5 - x * (1.0 / 6 - x * (1.0 / 24 - x * (1.0 / 120 - x / 720)))))
    return jnp.where(x < 0.25, series, 1.0 - jnp.exp(-x))


def expand(value):
    both = jnp.concatenate([value, value], axis=1)
    row, lane = iota((8, 128), 0), iota((8, 128), 1)
    parts = [
        jnp.sum(jnp.where(row == 2 * q + (lane >= 64).astype(jnp.int32), both, 0.0), axis=0, keepdims=True)
        for q in range(4)
    ]
    return jnp.concatenate(parts, axis=1)


def inclusive(a, s, backward):
    row = iota(s[0].shape, 0)
    for shift in (1, 2, 4):
        ok = row < 8 - shift if backward else row >= shift
        turn = 8 - shift if backward else shift
        pa = tuple(pltpu.roll(v, turn, 0) for v in a)
        ps = tuple(pltpu.roll(v, turn, 0) for v in s)
        na, ns = cmul(a, pa), cmul(a, ps)
        s = tuple(jnp.where(ok, n + o, o) for n, o in zip(ns, s))
        a = tuple(jnp.where(ok, n, o) for n, o in zip(na, a))
    return a, s


def exclusive(a, s, backward):
    row = iota(s[0].shape, 0)
    ok = row < 7 if backward else row >= 1
    turn = 7 if backward else 1
    ident = (1.0, 0.0)
    ea = tuple(jnp.where(ok, pltpu.roll(v, turn, 0), i) for v, i in zip(a, ident))
    es = tuple(jnp.where(ok, pltpu.roll(v, turn, 0), 0.0) for v in s)
    return ea, es


def product(g):
    for shift in (1, 2, 4):
        g = g * pltpu.roll(g, shift, 0)
    return g


def pick(value, index):
    row = iota(value.shape, 0)
    return jnp.sum(jnp.where(row == index, value, 0.0), axis=0, keepdims=True)


def kernel(
    residual, mixer_input, log_gate, decay_rate, turn_rate, drive_real, drive_imag, read_real,
    read_imag, skip_gain, project_hbm, norm_gain, final_gain, routes, group_weight, expert_weight,
    gate_hbm, linear_hbm, down_hbm,
    out,
    project, w_gate, w_linear, w_down,
    gates, push, msg1, recv1, msg2, recv2, act_out, act_in, middle, rows,
    out1, in1, out2, xin, gate_acc, linear_acc, hidden,
    opp_out, fwd_r, fwd_l, right_out, left_out, from_l, from_r, keep_r, keep_l,
    ans, b2in, b2out, b1in,
    w_sem, small_send, small_recv, yc_send, yc_recv, z_send, z_recv, x_send, x_recv, o_recv,
    rs_send, rs_recv,
):
    sp, x = lax.axis_index("sp"), lax.axis_index("tp")
    z, yc = sp // 8, lax.rem(sp, 8)
    right, left, opposite = lax.rem(x + 1, 4), lax.rem(x + 3, 4), lax.rem(x + 2, 4)

    def yc_peer(k):
        other = lax.rem(yc + k, 8)
        return other, (z * 8 + other, x)

    def z_peer(k):
        other = lax.rem(z + k, 8)
        return other, (other * 8 + yc, x)

    def send(src, dst, s_sem, r_sem, device):
        pltpu.make_async_remote_copy(
            src_ref=src, dst_ref=dst, send_sem=s_sem, recv_sem=r_sem,
            device_id=device, device_id_type=MESH,
        ).start()

    def settle(ref, sem):
        pltpu.make_async_copy(ref, ref, sem).wait()

    barrier = pltpu.get_barrier_semaphore()
    for k in range(1, 8):
        pl.semaphore_signal(barrier, inc=1, device_id=yc_peer(k)[1], device_id_type=MESH)
        pl.semaphore_signal(barrier, inc=1, device_id=z_peer(k)[1], device_id_type=MESH)
    for k in range(1, 4):
        pl.semaphore_signal(barrier, inc=1, device_id=(sp, lax.rem(x + k, 4)), device_id_type=MESH)

    loads = [
        pltpu.make_async_copy(project_hbm, project, w_sem.at[0]),
        pltpu.make_async_copy(gate_hbm, w_gate, w_sem.at[1]),
        pltpu.make_async_copy(linear_hbm, w_linear, w_sem.at[2]),
        pltpu.make_async_copy(down_hbm, w_down, w_sem.at[3]),
    ]
    for load in loads:
        load.start()

    r_id, t_id = iota((192, 192), 0), iota((192, 192), 1)
    order = (t_id == lax.rem(r_id, 8) * SEGMENT + r_id // 8).astype(F32).astype(BF16)
    order_back = (r_id == lax.rem(t_id, 8) * SEGMENT + t_id // 8).astype(F32).astype(BF16)
    inputs = dot(order, mixer_input[...])
    inputs_bf = inputs.astype(BF16)
    double = jnp.concatenate([inputs_bf, inputs_bf], axis=1)

    gate_rows = jnp.exp(log_gate[...])
    g1 = gate_rows.astype(BF16).astype(F32)
    g2 = (gate_rows - g1).astype(BF16).astype(F32)
    g3 = gate_rows - g1 - g2
    three = jnp.concatenate([g1, g2, g3], axis=0).astype(BF16)
    three = dot_nt(three, order).astype(BF16)
    widen = (lax.rem(iota((24, 512), 0), 8) == iota((24, 512), 1) // 64).astype(F32).astype(BF16)
    wide = dot_tn(three, widen)
    for q in range(4):
        gates[q] = wide[:, 128 * q : 128 * (q + 1)]

    step, power24, power192, power1536 = [], [], [], []
    scale = []
    for d in range(2):
        rate, turn = decay_rate[d], turn_rate[d]
        retain = jnp.exp(-rate)
        step.append((expand(retain * jnp.cos(turn)), expand(retain * jnp.sin(turn))))
        scale.append(expand(jnp.sqrt(one_minus_exp_neg(2.0 * rate))))
        p = step[d]
        for _ in range(3):
            p = cmul(p, p)
        p24 = cmul(cmul(p, p), p)
        power24.append(p24)
        p = p24
        for _ in range(3):
            p = cmul(p, p)
        power192.append(p)
        for _ in range(3):
            p = cmul(p, p)
        power1536.append(p)

    def block_diagonal(table, q):
        both = jnp.concatenate([table, table], axis=1)
        group = iota((128, 128), 0) // 16
        lane = iota((128, 128), 1)
        return jnp.where(group == 2 * q + (lane >= 64).astype(jnp.int32), both, 0.0)

    for d in range(2):
        for part, table_ref in enumerate((drive_real, drive_imag)):
            table = table_ref[pl.ds(128 * d, 128), :]
            for q in range(0, 4, 2):
                cols = jnp.concatenate([block_diagonal(table, q), block_diagonal(table, q + 1)], axis=1)
                high, low = halves(cols * scale[d][:, 128 * q : 128 * (q + 2)])
                pushed = dot(double, jnp.concatenate([high, low], axis=0))
                push[2 * d + part, q] = pushed[:, :128]
                push[2 * d + part, q + 1] = pushed[:, 128:]

    steps = [
        [
            tuple(jnp.broadcast_to(step[d][m][:, 128 * q : 128 * (q + 1)], (8, 128)) for m in range(2))
            for q in range(4)
        ]
        for d in range(2)
    ]

    def sweep(initial, final):
        def body(j, carried):
            states, decay = carried
            new = []
            new_decay = []
            for d in range(2):
                at = pl.multiple_of((j if d == 0 else SEGMENT - 1 - j) * 8, 8)
                for q in range(4):
                    re, im = states[2 * (4 * d + q)], states[2 * (4 * d + q) + 1]
                    g = gates[q, pl.ds(at, 8), :]
                    if d == 0 and not final:
                        new_decay.append(decay[q] * g)
                    sr, si = steps[d][q]
                    nr = g * (sr * re - si * im) + push[2 * d, q, pl.ds(at, 8), :]
                    ni = g * (sr * im + si * re) + push[2 * d + 1, q, pl.ds(at, 8), :]
                    if final:
                        push[2 * d, q, pl.ds(at, 8), :] = nr
                        push[2 * d + 1, q, pl.ds(at, 8), :] = ni
                    new += [nr, ni]
            return tuple(new), tuple(new_decay)

        ones = () if final else tuple(jnp.ones((8, 128), F32) for _ in range(4))
        return lax.fori_loop(0, SEGMENT, body, (initial, ones))

    zeros = tuple(jnp.zeros((8, 128), F32) for _ in range(16))
    ends, decay = sweep(zeros, False)
    decay = jnp.concatenate(decay, axis=1)
    enter = []
    for d in range(2):
        s = tuple(jnp.concatenate([ends[2 * (4 * d + q) + m] for q in range(4)], axis=1) for m in range(2))
        a = tuple(decay * p for p in power24[d])
        a, s = inclusive(a, s, d == 1)
        enter.append(exclusive(a, s, d == 1))
        last = 0 if d == 1 else 7
        for m in range(2):
            msg1[pl.ds(2 * d + m, 1), :] = s[m][last : last + 1, :]
    total_decay = product(decay)
    msg1[pl.ds(4, 4), :] = total_decay[0:4, :]

    pl.semaphore_wait(barrier, 17)

    def level(msg, recv, peer, me, index, powers):
        for k in range(1, 8):
            send(msg, recv.at[me], small_send.at[index], small_recv.at[index], peer(k)[1])
        recv[pl.ds(me, 1)] = msg[...][None]
        settle(recv.at[pl.ds(0, 7)], small_recv.at[index])
        decays = recv[:, 4, :]
        found = []
        for d in range(2):
            s = tuple(recv[:, 2 * d + m, :] for m in range(2))
            a = tuple(decays * p for p in powers[d])
            a, s = inclusive(a, s, d == 1)
            ea, es = exclusive(a, s, d == 1)
            last = 0 if d == 1 else 7
            found.append(
                (
                    tuple(pick(v, me) for v in ea),
                    tuple(pick(v, me) for v in es),
                    tuple(v[last : last + 1, :] for v in s),
                )
            )
        return found, product(decays)

    found1, plane_decay = level(msg1, recv1, yc_peer, yc, 0, power192)
    for d in range(2):
        for m in range(2):
            msg2[pl.ds(2 * d + m, 1), :] = found1[d][2][m]
    msg2[pl.ds(4, 4), :] = plane_decay[0:4, :]
    found2, _ = level(msg2, recv2, z_peer, z, 1, power1536)
    initial = []
    for d in range(2):
        pa, ps, _ = found1[d]
        carry = cmul(pa, found2[d][1])
        carry = tuple(c + p for c, p in zip(carry, ps))
        ea, es = enter[d]
        first = cmul(ea, carry)
        first = tuple(f + e for f, e in zip(first, es))
        for q in range(4):
            initial += [f[:, 128 * q : 128 * (q + 1)] for f in first]
    sweep(tuple(initial), True)

    readout = None
    for index in range(4):
        d, part = divmod(index, 2)
        table = (read_real, read_imag)[part][pl.ds(128 * d, 128), :]
        table = table if part == 0 else -table
        for q in range(0, 4, 2):
            s_high, s_low = halves(jnp.concatenate([push[index, q], push[index, q + 1]], axis=1))
            cols = jnp.concatenate([block_diagonal(table, q), block_diagonal(table, q + 1)], axis=1)
            r_high, r_low = halves(cols)
            term = dot_nt(s_high, r_high) + dot_nt(s_low, r_high) + dot_nt(s_high, r_low)
            readout = term if readout is None else readout + term
    readout = readout + skip_gain[...] * inputs
    inner = 0.7978845608028654 * (readout + 0.044715 * readout * readout * readout)
    activated = (0.5 * readout * (1.0 + jnp.tanh(inner))).astype(BF16)
    activated = dot(order_back, activated).astype(BF16)
    act_out[...] = activated.reshape(4, 48, 128)
    for k in range(1, 4):
        other = lax.rem(x + k, 4)
        send(act_out.at[other], act_in.at[x], small_send.at[2], small_recv.at[2], (sp, other))
    act_in[pl.ds(x, 1)] = act_out[pl.ds(x, 1)]

    chosen = routes[...].astype(F32)
    weights = expert_weight[...]
    mixing = group_weight[...] * weights / jnp.sum(weights, axis=0, keepdims=True)
    own = iota((192, 128), 0) == 48 * x + iota((192, 128), 1)
    own = (own & (iota((192, 128), 1) < 48)).astype(F32)
    chosen = jnp.dot(chosen, own, precision=lax.Precision.HIGHEST, preferred_element_type=F32)
    mixing = jnp.dot(mixing, own, precision=lax.Precision.HIGHEST, preferred_element_type=F32)
    slot, lane = iota((128, 128), 0), iota((128, 128), 1)
    expert = (lax.rem(slot, 16) // 2 * 8 + slot // 16).astype(F32)
    first = (chosen[0:1, :] == expert) & (lane < 48)
    second = (chosen[1:2, :] == expert) & (lane < 48)
    match = jnp.where(first | second, 1.0, 0.0)
    earlier = (slot < lane).astype(F32).astype(BF16)
    rank = dot(match.astype(BF16), earlier)
    taken = jnp.where(rank == lax.rem(slot, 2).astype(F32), match, 0.0)
    combine = taken * jnp.where(first, mixing[0:1, :], mixing[1:2, :])
    combine_high, combine_low = halves(combine.T)
    taken = taken.astype(BF16)
    r_id, c_id = slot, lane
    swapped = lax.rem(r_id, 16) // 2 * 16 + r_id // 16 * 2 + lax.rem(r_id, 2)
    swap = (c_id == swapped).astype(F32).astype(BF16)

    rows[pl.ds(48, 80), :] = jnp.zeros((80, CHUNKS * WIDE), BF16)
    loads[0].wait()
    settle(act_in.at[pl.ds(0, 3)], small_recv.at[2])
    channels = jnp.concatenate([act_in[m] for m in range(4)], axis=1)
    total = jnp.zeros((48, 1), F32)
    for c in range(CHUNKS):
        cols = pl.ds(WIDE * c, WIDE)
        v = deep_alpha * residual[:, cols].astype(F32) + dot(channels, project[:, cols])
        middle[:, cols] = v
        total = total + jnp.sum(v, axis=1, keepdims=True)
    mean = total / (CHUNKS * WIDE)
    total = jnp.zeros((48, 1), F32)
    for c in range(CHUNKS):
        center = middle[:, pl.ds(WIDE * c, WIDE)] - mean
        total = total + jnp.sum(center * center, axis=1, keepdims=True)
    factor = lax.rsqrt(total / (CHUNKS * WIDE) + norm_epsilon)
    for c in range(CHUNKS):
        cols = pl.ds(WIDE * c, WIDE)
        v = (middle[:, cols] - mean) * factor * norm_gain[:, cols]
        middle[:, cols] = v
        rows[pl.ds(0, 48), cols] = v.astype(BF16)
        out1[:, :, cols] = dot(taken, rows[:, cols]).astype(BF16).reshape(8, 16, WIDE)
        for k in range(1, 8):
            other, device = yc_peer(k)
            send(out1.at[other, :, cols], in1.at[yc, :, cols], yc_send.at[0], yc_recv.at[0, c], device)
        in1[pl.ds(yc, 1), :, cols] = out1[pl.ds(yc, 1), :, cols]

    for c in range(CHUNKS):
        cols = pl.ds(WIDE * c, WIDE)
        settle(in1.at[pl.ds(0, 7), :, cols], yc_recv.at[0, c])
        moved = dot(swap, in1[:, :, cols].reshape(128, WIDE)).astype(BF16)
        out2[:, :, cols] = moved.reshape(8, 16, WIDE)
        for k in range(1, 8):
            other, device = z_peer(k)
            send(out2.at[other, :, cols], xin.at[0, z, :, cols], z_send.at[0], z_recv.at[0, c], device)
        xin[0, pl.ds(z, 1), :, cols] = out2[pl.ds(z, 1), :, cols]

    low, high = pl.ds(0, 4), pl.ds(4, 4)

    def spread(c):
        cols = pl.ds(WIDE * c, WIDE)
        settle(xin.at[0, pl.ds(0, 7), :, cols], z_recv.at[0, c])
        send(xin.at[0, :, :, cols], xin.at[1, :, :, cols], x_send.at[0], x_recv.at[0, c], (sp, right))
        send(xin.at[0, :, :, cols], xin.at[2, :, :, cols], x_send.at[1], x_recv.at[1, c], (sp, left))

    def pass_on(c):
        cols = pl.ds(WIDE * c, WIDE)
        settle(xin.at[1, :, :, cols], x_recv.at[0, c])
        send(xin.at[1, low, :, cols], xin.at[3, low, :, cols], x_send.at[2], o_recv.at[0, c], (sp, right))
        settle(xin.at[2, :, :, cols], x_recv.at[1, c])
        send(xin.at[2, high, :, cols], xin.at[3, high, :, cols], x_send.at[3], o_recv.at[1, c], (sp, left))

    def multiply(c):
        cols = pl.ds(WIDE * c, WIDE)
        settle(xin.at[3, low, :, cols], o_recv.at[0, c])
        settle(xin.at[3, high, :, cols], o_recv.at[1, c])
        block = xin[:, :, :, cols].reshape(512, WIDE)
        for acc, weight in ((gate_acc, w_gate), (linear_acc, w_linear)):
            term = dot(block, weight[cols, :])
            acc[...] = term if c == 0 else acc[...] + term

    loads[1].wait()
    loads[2].wait()
    for c in range(CHUNKS + 2):
        if c < CHUNKS:
            spread(c)
        if 1 <= c <= CHUNKS:
            pass_on(c - 1)
        if c >= 2:
            multiply(c - 2)
    gate = gate_acc[...]
    hidden[...] = (gate / (1.0 + jnp.exp(-gate)) * linear_acc[...]).astype(BF16)
    loads[3].wait()

    def partial(source, c):
        part = dot(hidden[pl.ds(128 * source, 128), :], w_down[:, pl.ds(WIDE * c, WIDE)])
        return part.reshape(8, 16, WIDE)

    def start_sums(c):
        cols = pl.ds(WIDE * c, WIDE)
        opp_out[:, :, cols] = partial(3, c).astype(BF16)
        send(opp_out.at[low, :, cols], fwd_r.at[:, :, cols], rs_send.at[0], rs_recv.at[0, c], (sp, right))
        send(opp_out.at[high, :, cols], fwd_l.at[:, :, cols], rs_send.at[1], rs_recv.at[1, c], (sp, left))
        part = partial(2, c)
        right_out[high, :, cols] = part[4:8].astype(BF16)
        keep_r[:, :, cols] = part[0:4]
        send(right_out.at[high, :, cols], from_l.at[high, :, cols], rs_send.at[2], rs_recv.at[2, c], (sp, right))
        part = partial(1, c)
        left_out[low, :, cols] = part[0:4].astype(BF16)
        keep_l[:, :, cols] = part[4:8]
        send(left_out.at[low, :, cols], from_r.at[low, :, cols], rs_send.at[3], rs_recv.at[3, c], (sp, left))

    def add_on(c):
        cols = pl.ds(WIDE * c, WIDE)
        settle(fwd_r.at[:, :, cols], rs_recv.at[0, c])
        right_out[low, :, cols] = (keep_r[:, :, cols] + fwd_r[:, :, cols].astype(F32)).astype(BF16)
        send(right_out.at[low, :, cols], from_l.at[low, :, cols], rs_send.at[4], rs_recv.at[4, c], (sp, right))
        settle(fwd_l.at[:, :, cols], rs_recv.at[1, c])
        left_out[high, :, cols] = (keep_l[:, :, cols] + fwd_l[:, :, cols].astype(F32)).astype(BF16)
        send(left_out.at[high, :, cols], from_r.at[high, :, cols], rs_send.at[5], rs_recv.at[5, c], (sp, left))

    def finish_sums(c):
        cols = pl.ds(WIDE * c, WIDE)
        part = partial(0, c)
        settle(from_l.at[high, :, cols], rs_recv.at[2, c])
        settle(from_r.at[low, :, cols], rs_recv.at[3, c])
        settle(from_l.at[low, :, cols], rs_recv.at[4, c])
        settle(from_r.at[high, :, cols], rs_recv.at[5, c])
        part = part + from_l[:, :, cols].astype(F32) + from_r[:, :, cols].astype(F32)
        ans[:, :, cols] = part.astype(BF16)
        for k in range(1, 8):
            other, device = z_peer(k)
            send(ans.at[other, :, cols], b2in.at[z, :, cols], z_send.at[1], z_recv.at[1, c], device)
        b2in[pl.ds(z, 1), :, cols] = ans[pl.ds(z, 1), :, cols]

    def go_home(c):
        cols = pl.ds(WIDE * c, WIDE)
        settle(b2in.at[pl.ds(0, 7), :, cols], z_recv.at[1, c])
        moved = dot(swap, b2in[:, :, cols].reshape(128, WIDE)).astype(BF16)
        b2out[:, :, cols] = moved.reshape(8, 16, WIDE)
        for k in range(1, 8):
            other, device = yc_peer(k)
            send(b2out.at[other, :, cols], b1in.at[yc, :, cols], yc_send.at[1], yc_recv.at[1, c], device)
        b1in[pl.ds(yc, 1), :, cols] = b2out[pl.ds(yc, 1), :, cols]

    for c in range(CHUNKS + 3):
        if c < CHUNKS:
            start_sums(c)
        if 1 <= c <= CHUNKS:
            add_on(c - 1)
        if 2 <= c <= CHUNKS + 1:
            finish_sums(c - 2)
        if c >= 3:
            go_home(c - 3)

    total = jnp.zeros((48, 1), F32)
    for c in range(CHUNKS):
        cols = pl.ds(WIDE * c, WIDE)
        settle(b1in.at[pl.ds(0, 7), :, cols], yc_recv.at[1, c])
        back = b1in[:, :, cols].reshape(128, WIDE)
        routed = dot(combine_high, back) + dot(combine_low, back)
        v = deep_alpha * middle[:, cols] + routed[0:48, :]
        middle[:, cols] = v
        total = total + jnp.sum(v, axis=1, keepdims=True)
    mean = total / (CHUNKS * WIDE)
    total = jnp.zeros((48, 1), F32)
    for c in range(CHUNKS):
        center = middle[:, pl.ds(WIDE * c, WIDE)] - mean
        total = total + jnp.sum(center * center, axis=1, keepdims=True)
    factor = lax.rsqrt(total / (CHUNKS * WIDE) + norm_epsilon)
    for c in range(CHUNKS):
        cols = pl.ds(WIDE * c, WIDE)
        out[:, cols] = ((middle[:, cols] - mean) * factor * final_gain[:, cols]).astype(BF16)

    for index, recv in enumerate((recv1, recv2)):
        settle(recv.at[pl.ds(0, 7)], small_send.at[index])
    settle(act_in.at[pl.ds(0, 3)], small_send.at[2])
    for index in range(2):
        settle(out1.at[pl.ds(0, 7)], yc_send.at[index])
        settle(out2.at[pl.ds(0, 7)], z_send.at[index])
        settle(xin.at[0], x_send.at[index])
        settle(xin.at[0, low], x_send.at[2 + index])
    for index in range(6):
        settle(fwd_r, rs_send.at[index])


def on_device(
    residual, mixer_input, log_gate, decay_rate, turn_rate, drive_real, drive_imaginary, read_real,
    read_imaginary, skip_gain, project_weight, norm_gain, final_gain, routes, group_weight,
    expert_weight, gate_weight, linear_weight, down_weight,
):
    vmem = pl.BlockSpec(memory_space=pltpu.VMEM)
    hbm = pl.BlockSpec(memory_space=pl.ANY)
    dma = pltpu.SemaphoreType.DMA
    slab = pltpu.VMEM((8, 16, 2048), BF16)
    half = pltpu.VMEM((4, 16, 2048), BF16)
    return pl.pallas_call(
        kernel,
        out_shape=jax.ShapeDtypeStruct((48, 2048), BF16),
        in_specs=[vmem] * 10 + [hbm] + [vmem] * 5 + [hbm] * 3,
        out_specs=vmem,
        scratch_shapes=[
            pltpu.VMEM((512, 2048), BF16),
            pltpu.VMEM((2048, 256), BF16),
            pltpu.VMEM((2048, 256), BF16),
            pltpu.VMEM((256, 2048), BF16),
            pltpu.VMEM((4, 192, 128), F32),
            pltpu.VMEM((4, 4, 192, 128), F32),
            pltpu.VMEM((8, 512), F32),
            pltpu.VMEM((8, 8, 512), F32),
            pltpu.VMEM((8, 512), F32),
            pltpu.VMEM((8, 8, 512), F32),
            pltpu.VMEM((4, 48, 128), BF16),
            pltpu.VMEM((4, 48, 128), BF16),
            pltpu.VMEM((48, 2048), F32),
            pltpu.VMEM((128, 2048), BF16),
            slab, slab, slab,
            pltpu.VMEM((4, 8, 16, 2048), BF16),
            pltpu.VMEM((512, 256), F32),
            pltpu.VMEM((512, 256), F32),
            pltpu.VMEM((512, 256), BF16),
            slab, half, half,
            slab, slab, slab, slab,
            pltpu.VMEM((4, 16, 2048), F32),
            pltpu.VMEM((4, 16, 2048), F32),
            slab, slab, slab, slab,
            dma((4,)), dma((3,)), dma((3,)),
            dma((2,)), dma((2, CHUNKS)), dma((2,)), dma((2, CHUNKS)),
            dma((4,)), dma((2, CHUNKS)), dma((2, CHUNKS)),
            dma((6,)), dma((6, CHUNKS)),
        ],
        compiler_params=pltpu.CompilerParams(
            collective_id=0, has_side_effects=True, vmem_limit_bytes=60 * 1024 * 1024
        ),
        name="layer",
    )(
        residual, mixer_input, log_gate.T, decay_rate, turn_rate,
        drive_real.reshape(256, 64), drive_imaginary.reshape(256, 64),
        read_real.reshape(256, 64), read_imaginary.reshape(256, 64),
        skip_gain.reshape(1, 128), project_weight, norm_gain.reshape(1, 2048),
        final_gain.reshape(1, 2048), routes.T, group_weight.reshape(1, 192), expert_weight.T,
        gate_weight[0], linear_weight[0], down_weight[0],
    )


def solution(mesh):
    placed = (
        P(("sp", "tp"), None),
        P("sp", "tp"),
        P("sp", "tp"),
        P(None, "tp", None),
        P(None, "tp", None),
        P(None, "tp", None, None),
        P(None, "tp", None, None),
        P(None, "tp", None, None),
        P(None, "tp", None, None),
        P("tp"),
        P(),
        P(),
        P(),
        P("sp", None),
        P("sp"),
        P("sp", None),
        P("sp", None, "tp"),
        P("sp", None, "tp"),
        P("sp", "tp", None),
    )
    return jax.shard_map(
        on_device, mesh=mesh, in_specs=placed, out_specs=P(("sp", "tp"), None), check_vma=False
    )
```

```python
import jax
import jax.numpy as jnp
from jax import lax
from jax.experimental import pallas as pl
from jax.experimental.pallas import tpu as pltpu
from jax.sharding import PartitionSpec as P

MESH = pl.DeviceIdType.MESH
F32 = jnp.float32
BF16 = jnp.bfloat16
deep_alpha = 2.0**0.25
norm_epsilon = 1e-05
SEGMENT = 24
CHUNKS = 4
WIDE = 512
HALF = 1024
ORDER = (0, 1, 7, 2, 6, 3, 5, 4)
LANDS = tuple(ORDER.index((8 - k) % 8) for k in ORDER)


def iota(shape, dim):
    return lax.broadcasted_iota(jnp.int32, shape, dim)


def cmul(a, b):
    return (a[0] * b[0] - a[1] * b[1], a[0] * b[1] + a[1] * b[0])


def dot(a, b):
    return jnp.dot(a, b, preferred_element_type=F32)


def dot_nt(a, b):
    return lax.dot_general(a, b, (((1,), (1,)), ((), ())), preferred_element_type=F32)


def dot_tn(a, b):
    return lax.dot_general(a, b, (((0,), (0,)), ((), ())), preferred_element_type=F32)


def halves(value):
    high = value.astype(BF16)
    return high, (value - high.astype(F32)).astype(BF16)


def one_minus_exp_neg(x):
    series = x * (1.0 - x * (0.5 - x * (1.0 / 6 - x * (1.0 / 24 - x * (1.0 / 120 - x / 720)))))
    return jnp.where(x < 0.25, series, 1.0 - jnp.exp(-x))


def expand(value):
    both = jnp.concatenate([value, value], axis=1)
    row, lane = iota((8, 128), 0), iota((8, 128), 1)
    parts = [
        jnp.sum(jnp.where(row == 2 * q + (lane >= 64).astype(jnp.int32), both, 0.0), axis=0, keepdims=True)
        for q in range(4)
    ]
    return jnp.concatenate(parts, axis=1)


def inclusive(a, s, backward):
    row = iota(s[0].shape, 0)
    for shift in (1, 2, 4):
        ok = row < 8 - shift if backward else row >= shift
        turn = 8 - shift if backward else shift
        pa = tuple(pltpu.roll(v, turn, 0) for v in a)
        ps = tuple(pltpu.roll(v, turn, 0) for v in s)
        na, ns = cmul(a, pa), cmul(a, ps)
        s = tuple(jnp.where(ok, n + o, o) for n, o in zip(ns, s))
        a = tuple(jnp.where(ok, n, o) for n, o in zip(na, a))
    return a, s


def exclusive(a, s, backward):
    row = iota(s[0].shape, 0)
    ok = row < 7 if backward else row >= 1
    turn = 7 if backward else 1
    ident = (1.0, 0.0)
    ea = tuple(jnp.where(ok, pltpu.roll(v, turn, 0), i) for v, i in zip(a, ident))
    es = tuple(jnp.where(ok, pltpu.roll(v, turn, 0), 0.0) for v in s)
    return ea, es


def product(g):
    for shift in (1, 2, 4):
        g = g * pltpu.roll(g, shift, 0)
    return g


def pick(value, index):
    row = iota(value.shape, 0)
    return jnp.sum(jnp.where(row == index, value, 0.0), axis=0, keepdims=True)


INPUTS = (
    ((48, 2048), BF16), ((192, 128), BF16), ((8, 192), F32), ((2, 8, 64), F32), ((2, 8, 64), F32),
    ((256, 64), F32), ((256, 64), F32), ((256, 64), F32), ((256, 64), F32), ((1, 128), F32),
    ((512, 2048), BF16), ((1, 2048), F32), ((2, 192), jnp.int32), ((1, 192), F32), ((2, 192), F32),
    ((2048, 256), BF16), ((2048, 256), BF16), ((256, 2048), BF16),
)


def kernel(*refs):
    count = len(INPUTS)
    sources, out, held = refs[:count], refs[count], refs[count + 1 : 2 * count + 1]
    (
        residual, mixer_input, log_gate, decay_rate, turn_rate, drive_real, drive_imag, read_real,
        read_imag, skip_gain, project, norm_gain, routes, group_weight, expert_weight,
        w_gate, w_linear, w_down,
    ) = held
    (
        gates, push, msg1, recv1, msg2, recv2, act_out, act_in, middle, rows, tables, taken, combine,
        swap, out1, in1, out2, xin, hidden, opp_out, fwd_r, fwd_l, right_out, left_out, from_l,
        from_r, keep_r, keep_l, keep_o, ans, b2in, b2out, b1in,
        w_sem, small_send, small_recv, yc_send, yc_recv, z_send, z_recv, z_back, x_send, x_recv,
        o_recv, rs_send, rs_recv,
    ) = refs[2 * count + 1 :]
    sp, x = lax.axis_index("sp"), lax.axis_index("tp")
    z, yc = sp // 8, lax.rem(sp, 8)
    right, left = lax.rem(x + 1, 4), lax.rem(x + 3, 4)

    def yc_peer(k):
        other = lax.rem(yc + k, 8)
        return other, (z * 8 + other, x)

    def z_peer(k):
        other = lax.rem(z + k, 8)
        return other, (other * 8 + yc, x)

    def send(src, dst, s_sem, r_sem, device):
        pltpu.make_async_remote_copy(
            src_ref=src, dst_ref=dst, send_sem=s_sem, recv_sem=r_sem,
            device_id=device, device_id_type=MESH,
        ).start()

    def settle(ref, sem):
        pltpu.make_async_copy(ref, ref, sem).wait()

    barrier = pltpu.get_barrier_semaphore()
    for k in (4, 3, 5, 2, 6, 1, 7):
        pl.semaphore_signal(barrier, inc=1, device_id=z_peer(k)[1], device_id_type=MESH)
    for k in range(1, 8):
        pl.semaphore_signal(barrier, inc=1, device_id=yc_peer(k)[1], device_id_type=MESH)
    for k in range(1, 4):
        pl.semaphore_signal(barrier, inc=1, device_id=(sp, lax.rem(x + k, 4)), device_id_type=MESH)
    loads = [pltpu.make_async_copy(a, b, w_sem.at[n]) for n, (a, b) in enumerate(zip(sources, held))]
    first_needed = (1, 2, 3, 4, 5, 6)
    for n in first_needed:
        loads[n].start()
    for n in range(count):
        if n not in first_needed:
            loads[n].start()
    for n in first_needed:
        loads[n].wait()

    r_id, t_id = iota((192, 192), 0), iota((192, 192), 1)
    order = (t_id == lax.rem(r_id, 8) * SEGMENT + r_id // 8).astype(F32).astype(BF16)
    inputs_bf = dot(order, mixer_input[...]).astype(BF16)
    double = jnp.concatenate([inputs_bf, inputs_bf], axis=1)

    gate_rows = jnp.exp(log_gate[...])
    g1 = gate_rows.astype(BF16).astype(F32)
    g2 = (gate_rows - g1).astype(BF16).astype(F32)
    g3 = gate_rows - g1 - g2
    three = jnp.concatenate([g1, g2, g3], axis=0).astype(BF16)
    three = dot_nt(three, order).astype(BF16)
    widen = (lax.rem(iota((24, 512), 0), 8) == iota((24, 512), 1) // 64).astype(F32).astype(BF16)
    wide = dot_tn(three, widen)
    for q in range(4):
        gates[q] = wide[:, 128 * q : 128 * (q + 1)]

    step, power24, power192, power1536 = [], [], [], []
    scale = []
    for d in range(2):
        rate, turn = decay_rate[d], turn_rate[d]
        retain = jnp.exp(-rate)
        step.append((expand(retain * jnp.cos(turn)), expand(retain * jnp.sin(turn))))
        scale.append(expand(jnp.sqrt(one_minus_exp_neg(2.0 * rate))))
        p = step[d]
        for _ in range(3):
            p = cmul(p, p)
        p24 = cmul(cmul(p, p), p)
        power24.append(p24)
        p = p24
        for _ in range(3):
            p = cmul(p, p)
        power192.append(p)
        for _ in range(3):
            p = cmul(p, p)
        power1536.append(p)

    def block_diagonal(table, q):
        both = jnp.concatenate([table, table], axis=1)
        group = iota((128, 128), 0) // 16
        lane = iota((128, 128), 1)
        return jnp.where(group == 2 * q + (lane >= 64).astype(jnp.int32), both, 0.0)

    def pair(table, q):
        return jnp.concatenate([block_diagonal(table, q), block_diagonal(table, q + 1)], axis=1)

    for d in range(2):
        for part, table_ref in enumerate((drive_real, drive_imag)):
            table = table_ref[pl.ds(128 * d, 128), :]
            for q in range(0, 4, 2):
                high, low = halves(pair(table, q) * scale[d][:, 128 * q : 128 * (q + 2)])
                pushed = dot(double, jnp.concatenate([high, low], axis=0))
                push[2 * d + part, q] = pushed[:, :128]
                push[2 * d + part, q + 1] = pushed[:, 128:]

    steps = [
        [
            tuple(jnp.broadcast_to(step[d][m][:, 128 * q : 128 * (q + 1)], (8, 128)) for m in range(2))
            for q in range(4)
        ]
        for d in range(2)
    ]

    def sweep(initial, final):
        def body(j, carried):
            states, decay = carried
            new = []
            new_decay = []
            for d in range(2):
                at = pl.multiple_of((j if d == 0 else SEGMENT - 1 - j) * 8, 8)
                for q in range(4):
                    re, im = states[2 * (4 * d + q)], states[2 * (4 * d + q) + 1]
                    g = gates[q, pl.ds(at, 8), :]
                    if d == 0 and not final:
                        new_decay.append(decay[q] * g)
                    sr, si = steps[d][q]
                    nr = g * (sr * re - si * im) + push[2 * d, q, pl.ds(at, 8), :]
                    ni = g * (sr * im + si * re) + push[2 * d + 1, q, pl.ds(at, 8), :]
                    if final:
                        push[2 * d, q, pl.ds(at, 8), :] = nr
                        push[2 * d + 1, q, pl.ds(at, 8), :] = ni
                    new += [nr, ni]
            return tuple(new), tuple(new_decay)

        ones = () if final else tuple(jnp.ones((8, 128), F32) for _ in range(4))
        return lax.fori_loop(0, SEGMENT, body, (initial, ones))

    def put(msg, d, m, row):
        for q in range(4):
            msg[2 * d, pl.ds(4 * m + q, 1), :] = row[:, 128 * q : 128 * (q + 1)]

    def put_decay(msg, value):
        for q in range(4):
            msg[1, pl.ds(q, 1), :] = value[0:1, 128 * q : 128 * (q + 1)]
            msg[1, pl.ds(4 + q, 1), :] = value[0:1, 128 * q : 128 * (q + 1)]

    zeros = tuple(jnp.zeros((8, 128), F32) for _ in range(16))
    ends, decay = sweep(zeros, False)
    decay = jnp.concatenate(decay, axis=1)
    enter = []
    for d in range(2):
        s = tuple(jnp.concatenate([ends[2 * (4 * d + q) + m] for q in range(4)], axis=1) for m in range(2))
        a = tuple(decay * p for p in power24[d])
        a, s = inclusive(a, s, d == 1)
        enter.append(exclusive(a, s, d == 1))
        last = 0 if d == 1 else 7
        for m in range(2):
            put(msg1, d, m, s[m][last : last + 1, :])
    put_decay(msg1, product(decay))

    pl.semaphore_wait(barrier, 17)

    def gathered(recv, slab, first_row):
        return jnp.concatenate([recv[:, slab, first_row + q, :] for q in range(4)], axis=1)

    def combined(recv, me, powers, masked):
        decays = gathered(recv, 1, 0)
        row = iota((8, 512), 0)
        found = []
        for d in range(2):
            s = tuple(gathered(recv, 2 * d, 4 * m) for m in range(2))
            if masked:
                used = row > me if d == 1 else row < me
                s = tuple(jnp.where(used, v, 0.0) for v in s)
            a = tuple(decays * p for p in powers[d])
            a, s = inclusive(a, s, d == 1)
            ea, es = exclusive(a, s, d == 1)
            last = 0 if d == 1 else 7
            found.append(
                (
                    tuple(pick(v, me) for v in ea),
                    tuple(pick(v, me) for v in es),
                    tuple(v[last : last + 1, :] for v in s),
                )
            )
        return found, decays

    for k in range(1, 8):
        send(msg1, recv1.at[yc], small_send.at[0], small_recv.at[0], yc_peer(k)[1])
    recv1[pl.ds(yc, 1)] = msg1[...][None]

    for n in (7, 8, 12, 13, 14):
        loads[n].wait()
    for index in range(4):
        d, part = divmod(index, 2)
        table = (read_real, read_imag)[part][pl.ds(128 * d, 128), :]
        table = table if part == 0 else -table
        for q in range(0, 4, 2):
            tables[index, q // 2] = jnp.concatenate(halves(pair(table, q)), axis=0)
    chosen = routes[...].astype(F32)
    weights = expert_weight[...]
    mixing = group_weight[...] * weights / jnp.sum(weights, axis=0, keepdims=True)
    own = iota((192, 128), 0) == 48 * x + iota((192, 128), 1)
    own = (own & (iota((192, 128), 1) < 48)).astype(F32)
    chosen = jnp.dot(chosen, own, precision=lax.Precision.HIGHEST, preferred_element_type=F32)
    mixing = jnp.dot(mixing, own, precision=lax.Precision.HIGHEST, preferred_element_type=F32)
    slot, lane = iota((128, 128), 0), iota((128, 128), 1)
    place = lax.rem(slot, 16) // 2
    offset = jnp.zeros_like(place)
    for i in range(1, 8):
        offset = jnp.where(place == i, ORDER[i], offset)
    expert = (lax.rem(z + offset, 8) * 8 + slot // 16).astype(F32)
    first = (chosen[0:1, :] == expert) & (lane < 48)
    second = (chosen[1:2, :] == expert) & (lane < 48)
    match = jnp.where(first | second, 1.0, 0.0)
    earlier = (slot < lane).astype(F32).astype(BF16)
    rank = dot(match.astype(BF16), earlier)
    mine = jnp.where(rank == lax.rem(slot, 2).astype(F32), match, 0.0)
    taken[...] = mine.astype(BF16)
    mine = mine * jnp.where(first, mixing[0:1, :], mixing[1:2, :])
    combine[0], combine[1] = halves(mine.T)
    swapped = place * 16 + slot // 16 * 2 + lax.rem(slot, 2)
    swap[...] = (lane == swapped).astype(F32).astype(BF16)
    rows[pl.ds(48, 80), :] = jnp.zeros((80, CHUNKS * WIDE), BF16)

    settle(recv1.at[pl.ds(0, 7)], small_recv.at[0])
    found1, decays = combined(recv1, yc, power192, False)
    for d in range(2):
        for m in range(2):
            put(msg2, d, m, found1[d][2][m])
    put_decay(msg2, product(decays))
    for k in (4, 3, 5, 2, 6, 1, 7):
        other, device = z_peer(k)
        part = pl.ds(jnp.where(other > z, 0, 1), 2)
        send(msg2.at[part], recv2.at[z, part], small_send.at[1], small_recv.at[1], device)
    recv2[pl.ds(z, 1)] = msg2[...][None]
    settle(recv2.at[pl.ds(0, 7), pl.ds(0, 2)], small_recv.at[1])
    found2, _ = combined(recv2, z, power1536, True)
    initial = []
    for d in range(2):
        pa, ps, _ = found1[d]
        carry = cmul(pa, found2[d][1])
        carry = tuple(c + p for c, p in zip(carry, ps))
        ea, es = enter[d]
        begin = cmul(ea, carry)
        begin = tuple(f + e for f, e in zip(begin, es))
        for q in range(4):
            initial += [f[:, 128 * q : 128 * (q + 1)] for f in begin]
    sweep(tuple(initial), True)

    loads[9].wait()
    readout = skip_gain[...] * inputs_bf.astype(F32)
    both = jnp.zeros((192, 256), F32)
    for index in range(4):
        for q in range(0, 4, 2):
            s_high, s_low = halves(jnp.concatenate([push[index, q], push[index, q + 1]], axis=1))
            both = both + dot_nt(s_high, tables[index, q // 2])
            readout = readout + dot_nt(s_low, tables[index, q // 2, pl.ds(0, 128), :])
    readout = readout + both[:, :128] + both[:, 128:]
    inner = 0.7978845608028654 * (readout + 0.044715 * readout * readout * readout)
    activated = (0.5 * readout * (1.0 + jnp.tanh(inner))).astype(BF16)
    r_id, t_id = iota((192, 192), 0), iota((192, 192), 1)
    order_back = (r_id == lax.rem(t_id, 8) * SEGMENT + t_id // 8).astype(F32).astype(BF16)
    activated = dot(order_back, activated).astype(BF16)
    act_out[...] = activated.reshape(4, 48, 128)
    for k in (2, 1, 3):
        other = lax.rem(x + k, 4)
        send(act_out.at[other], act_in.at[x], small_send.at[2], small_recv.at[2], (sp, other))
    act_in[pl.ds(x, 1)] = act_out[pl.ds(x, 1)]

    for n in (0, 10, 11):
        loads[n].wait()
    settle(act_in.at[pl.ds(0, 3)], small_recv.at[2])
    channels = jnp.concatenate([act_in[m] for m in range(4)], axis=1)
    total = jnp.zeros((48, 1), F32)
    for c in range(CHUNKS):
        cols = pl.ds(WIDE * c, WIDE)
        v = deep_alpha * residual[:, cols].astype(F32) + dot(channels, project[:, cols])
        middle[:, cols] = v
        total = total + jnp.sum(v, axis=1, keepdims=True)
    mean = total / (CHUNKS * WIDE)
    total = jnp.zeros((48, 1), F32)
    for c in range(CHUNKS):
        center = middle[:, pl.ds(WIDE * c, WIDE)] - mean
        total = total + jnp.sum(center * center, axis=1, keepdims=True)
    factor = lax.rsqrt(total / (CHUNKS * WIDE) + norm_epsilon)
    for c in range(CHUNKS):
        cols = pl.ds(WIDE * c, WIDE)
        v = (middle[:, cols] - mean) * factor * norm_gain[:, cols]
        middle[:, cols] = v
        rows[pl.ds(0, 48), cols] = v.astype(BF16)
        out1[:, :, cols] = dot(taken[...], rows[:, cols]).astype(BF16).reshape(8, 16, WIDE)
        for k in range(1, 8):
            other, device = yc_peer(k)
            send(out1.at[other, :, cols], in1.at[yc, :, cols], yc_send.at[0], yc_recv.at[0, c], device)
        in1[pl.ds(yc, 1), :, cols] = out1[pl.ds(yc, 1), :, cols]

    def side(h):
        return pl.ds(HALF * h, HALF)

    def start_z(i, h, cols):
        to = LANDS[i]
        send(
            out2.at[i, :, cols], xin.at[0, to, :, cols], z_send.at[0], z_recv.at[to, h],
            z_peer(ORDER[i])[1],
        )

    def spread(i, h, cols):
        block = xin.at[0, i, :, cols]
        rest = o_recv.at[i // 4]
        send(block, xin.at[1, i, :, cols], x_send.at[0], rest if h else x_recv.at[0, i], (sp, right))
        send(block, xin.at[2, i, :, cols], x_send.at[1], x_recv.at[1, i] if h else rest, (sp, left))

    def pass_on(i):
        block = xin.at[1, i, :, side(0)]
        settle(block, x_recv.at[0, i])
        send(block, xin.at[3, i, :, side(0)], x_send.at[2], o_recv.at[i // 4], (sp, right))
        block = xin.at[2, i, :, side(1)]
        settle(block, x_recv.at[1, i])
        send(block, xin.at[3, i, :, side(1)], x_send.at[3], o_recv.at[i // 4], (sp, left))

    for c in range(CHUNKS):
        cols = pl.ds(WIDE * c, WIDE)
        settle(in1.at[pl.ds(0, 7), :, cols], yc_recv.at[0, c])
        moved = dot(swap[...], in1[:, :, cols].reshape(128, WIDE)).astype(BF16)
        out2[:, :, cols] = moved.reshape(8, 16, WIDE)
        xin[0, 0, :, cols] = moved[0:16, :]
        for i in range(1, 4):
            start_z(i, c // 2, cols)
        spread(0, c // 2, cols)
    for i in range(4, 8):
        for h in range(2):
            start_z(i, h, side(h))

    def multiply(g):
        settle(xin.at[pl.ds(2, 2), pl.ds(4 * g, 4)], o_recv.at[g])
        block = xin[:, pl.ds(4 * g, 4)].reshape(256, 2048)
        gate = dot(block, w_gate[...])
        linear = dot(block, w_linear[...])
        hidden[g] = (gate / (1.0 + jnp.exp(-gate)) * linear).astype(BF16)

    low, high = pl.ds(0, 2), pl.ds(2, 2)

    def start_sums(g, c):
        cols = pl.ds(WIDE * c, WIDE)
        part = dot(hidden[g], w_down[:, cols]).reshape(4, 4, 16, WIDE)
        opp_out[g, :, :, cols] = part[3].astype(BF16)
        send(opp_out.at[g, low, :, cols], fwd_r.at[g, :, :, cols], rs_send.at[0], rs_recv.at[0, g, c], (sp, right))
        send(opp_out.at[g, high, :, cols], fwd_l.at[g, :, :, cols], rs_send.at[1], rs_recv.at[1, g, c], (sp, left))
        right_out[g, high, :, cols] = part[2, 2:4].astype(BF16)
        keep_r[g, :, :, cols] = part[2, 0:2]
        send(right_out.at[g, high, :, cols], from_l.at[g, high, :, cols], rs_send.at[2], rs_recv.at[2, g, c], (sp, right))
        left_out[g, low, :, cols] = part[1, 0:2].astype(BF16)
        keep_l[g, :, :, cols] = part[1, 2:4]
        send(left_out.at[g, low, :, cols], from_r.at[g, low, :, cols], rs_send.at[3], rs_recv.at[3, g, c], (sp, left))
        keep_o[g, :, :, cols] = part[0]

    def add_on(g, c):
        cols = pl.ds(WIDE * c, WIDE)
        settle(fwd_r.at[g, :, :, cols], rs_recv.at[0, g, c])
        right_out[g, low, :, cols] = (keep_r[g, :, :, cols] + fwd_r[g, :, :, cols].astype(F32)).astype(BF16)
        send(right_out.at[g, low, :, cols], from_l.at[g, low, :, cols], rs_send.at[2], rs_recv.at[2, g, c], (sp, right))
        settle(fwd_l.at[g, :, :, cols], rs_recv.at[1, g, c])
        left_out[g, high, :, cols] = (keep_l[g, :, :, cols] + fwd_l[g, :, :, cols].astype(F32)).astype(BF16)
        send(left_out.at[g, high, :, cols], from_r.at[g, high, :, cols], rs_send.at[3], rs_recv.at[3, g, c], (sp, left))

    def finish_sums(g, c):
        cols = pl.ds(WIDE * c, WIDE)
        settle(from_l.at[g, :, :, cols], rs_recv.at[2, g, c])
        settle(from_r.at[g, :, :, cols], rs_recv.at[3, g, c])
        part = keep_o[g, :, :, cols] + from_l[g, :, :, cols].astype(F32) + from_r[g, :, :, cols].astype(F32)
        ans[pl.ds(4 * g, 4), :, cols] = part.astype(BF16)
        for i in range(4 * g, 4 * g + 4):
            if i == 0:
                b2in[0, :, cols] = ans[0, :, cols]
                continue
            send(ans.at[i, :, cols], b2in.at[LANDS[i], :, cols], z_send.at[1], z_back.at[c], z_peer(ORDER[i])[1])

    def go_home(c):
        cols = pl.ds(WIDE * c, WIDE)
        settle(b2in.at[pl.ds(0, 7), :, cols], z_back.at[c])
        moved = dot(swap[...], b2in[:, :, cols].reshape(128, WIDE)).astype(BF16)
        b2out[:, :, cols] = moved.reshape(8, 16, WIDE)
        for k in range(1, 8):
            other, device = yc_peer(k)
            send(b2out.at[other, :, cols], b1in.at[yc, :, cols], yc_send.at[1], yc_recv.at[1, c], device)
        b1in[pl.ds(yc, 1), :, cols] = b2out[pl.ds(yc, 1), :, cols]

    for i in range(1, 8):
        for h in range(2):
            settle(xin.at[0, i, :, side(h)], z_recv.at[i, h])
            spread(i, h, side(h))
        pass_on(i - 1)
        if i == 1:
            for n in (15, 16, 17):
                loads[n].wait()
    multiply(0)
    pass_on(7)
    start_sums(0, 0)
    start_sums(0, 1)
    start_sums(0, 2)
    add_on(0, 0)
    multiply(1)
    start_sums(1, 0)
    start_sums(1, 1)
    add_on(0, 1)
    start_sums(1, 2)
    add_on(1, 0)
    start_sums(1, 3)
    add_on(1, 1)
    finish_sums(0, 0)
    finish_sums(0, 1)
    add_on(1, 2)
    finish_sums(1, 0)
    add_on(1, 3)
    start_sums(0, 3)
    finish_sums(1, 1)
    add_on(0, 2)
    finish_sums(1, 2)
    add_on(0, 3)
    finish_sums(1, 3)
    go_home(0)
    finish_sums(0, 2)
    finish_sums(0, 3)
    for c in range(1, CHUNKS):
        go_home(c)

    total = jnp.zeros((48, 1), F32)
    for c in range(CHUNKS):
        cols = pl.ds(WIDE * c, WIDE)
        settle(b1in.at[pl.ds(0, 7), :, cols], yc_recv.at[1, c])
        back = b1in[:, :, cols].reshape(128, WIDE)
        routed = dot(combine[0, pl.ds(0, 48), :], back) + dot(combine[1, pl.ds(0, 48), :], back)
        v = deep_alpha * middle[:, cols] + routed
        middle[:, cols] = v
        total = total + jnp.sum(v, axis=1, keepdims=True)
    mean = total / (CHUNKS * WIDE)
    total = jnp.zeros((48, 1), F32)
    for c in range(CHUNKS):
        center = middle[:, pl.ds(WIDE * c, WIDE)] - mean
        total = total + jnp.sum(center * center, axis=1, keepdims=True)
    factor = lax.rsqrt(total / (CHUNKS * WIDE) + norm_epsilon)
    for c in range(CHUNKS):
        cols = pl.ds(WIDE * c, WIDE)
        out[:, cols] = (middle[:, cols] - mean) * factor

    settle(recv1.at[pl.ds(0, 7)], small_send.at[0])
    settle(recv2.at[pl.ds(0, 7), pl.ds(0, 2)], small_send.at[1])
    settle(act_in.at[pl.ds(0, 3)], small_send.at[2])
    for index in range(2):
        settle(out1.at[pl.ds(0, 7)], yc_send.at[index])
        settle(out2.at[pl.ds(0, 7)], z_send.at[index])
        settle(xin.at[0], x_send.at[index])
        settle(xin.at[0, pl.ds(0, 4)], x_send.at[2 + index])
        settle(fwd_r, rs_send.at[index])
        settle(from_l, rs_send.at[2 + index])


def on_device(
    residual, mixer_input, log_gate, decay_rate, turn_rate, drive_real, drive_imaginary, read_real,
    read_imaginary, skip_gain, project_weight, norm_gain, final_gain, routes, group_weight,
    expert_weight, gate_weight, linear_weight, down_weight,
):
    dma = pltpu.SemaphoreType.DMA
    slab = pltpu.VMEM((8, 16, 2048), BF16)
    groups = pltpu.VMEM((2, 4, 16, 2048), BF16)
    half = pltpu.VMEM((2, 2, 16, 2048), BF16)
    normed = pl.pallas_call(
        kernel,
        out_shape=jax.ShapeDtypeStruct((48, 2048), F32),
        in_specs=[pl.BlockSpec(memory_space=pl.ANY)] * len(INPUTS),
        out_specs=pl.BlockSpec(memory_space=pltpu.VMEM),
        scratch_shapes=[pltpu.VMEM(shape, dtype) for shape, dtype in INPUTS]
        + [
            pltpu.VMEM((4, 192, 128), F32),
            pltpu.VMEM((4, 4, 192, 128), F32),
            pltpu.VMEM((3, 8, 128), F32),
            pltpu.VMEM((8, 3, 8, 128), F32),
            pltpu.VMEM((3, 8, 128), F32),
            pltpu.VMEM((8, 3, 8, 128), F32),
            pltpu.VMEM((4, 48, 128), BF16),
            pltpu.VMEM((4, 48, 128), BF16),
            pltpu.VMEM((48, 2048), F32),
            pltpu.VMEM((128, 2048), BF16),
            pltpu.VMEM((4, 2, 256, 256), BF16),
            pltpu.VMEM((128, 128), BF16),
            pltpu.VMEM((2, 128, 128), BF16),
            pltpu.VMEM((128, 128), BF16),
            slab, slab, slab,
            pltpu.VMEM((4, 8, 16, 2048), BF16),
            pltpu.VMEM((2, 256, 256), BF16),
            groups, half, half,
            groups, groups, groups, groups,
            pltpu.VMEM((2, 2, 16, 2048), F32),
            pltpu.VMEM((2, 2, 16, 2048), F32),
            pltpu.VMEM((2, 4, 16, 2048), F32),
            slab, slab, slab, slab,
            dma((len(INPUTS),)), dma((3,)), dma((3,)),
            dma((2,)), dma((2, CHUNKS)), dma((2,)), dma((8, 2)), dma((CHUNKS,)),
            dma((4,)), dma((2, 8)), dma((2,)),
            dma((4,)), dma((4, 2, CHUNKS)),
        ],
        compiler_params=pltpu.CompilerParams(
            collective_id=0, has_side_effects=True, vmem_limit_bytes=40 * 1024 * 1024
        ),
        name="layer",
    )(*(pltpu.with_memory_space_constraint(v, pltpu.HBM) for v in (
        residual, mixer_input, log_gate.T, decay_rate, turn_rate,
        drive_real.reshape(256, 64), drive_imaginary.reshape(256, 64),
        read_real.reshape(256, 64), read_imaginary.reshape(256, 64),
        skip_gain.reshape(1, 128), project_weight, norm_gain.reshape(1, 2048),
        routes.T, group_weight.reshape(1, 192), expert_weight.T,
        gate_weight[0], linear_weight[0], down_weight[0],
    )))
    return (normed * final_gain).astype(BF16)


def solution(mesh):
    placed = (
        P(("sp", "tp"), None),
        P("sp", "tp"),
        P("sp", "tp"),
        P(None, "tp", None),
        P(None, "tp", None),
        P(None, "tp", None, None),
        P(None, "tp", None, None),
        P(None, "tp", None, None),
        P(None, "tp", None, None),
        P("tp"),
        P(),
        P(),
        P(),
        P("sp", None),
        P("sp"),
        P("sp", None),
        P("sp", None, "tp"),
        P("sp", None, "tp"),
        P("sp", "tp", None),
    )
    return jax.shard_map(
        on_device, mesh=mesh, in_specs=placed, out_specs=P(("sp", "tp"), None), check_vma=False
    )
```

```python
import jax
import jax.numpy as jnp
from jax import lax
from jax.experimental import pallas as pl
from jax.experimental.pallas import tpu as pltpu
from jax.sharding import PartitionSpec as P

MESH = pl.DeviceIdType.MESH
F32 = jnp.float32
BF16 = jnp.bfloat16
deep_alpha = 2.0**0.25
norm_epsilon = 1e-05
SEGMENT = 24
CHUNKS = 4
WIDE = 512
HALF = 1024
FAR = (4, 3, 5, 2, 6, 1, 7)
ORDER = (0, 1, 7, 2, 6, 3, 5, 4)
LANDS = tuple(ORDER.index((8 - k) % 8) for k in ORDER)


def iota(shape, dim):
    return lax.broadcasted_iota(jnp.int32, shape, dim)


def cmul(a, b):
    return (a[0] * b[0] - a[1] * b[1], a[0] * b[1] + a[1] * b[0])


def dot(a, b):
    return jnp.dot(a, b, preferred_element_type=F32)


def dot_nt(a, b):
    return lax.dot_general(a, b, (((1,), (1,)), ((), ())), preferred_element_type=F32)


def dot_tn(a, b):
    return lax.dot_general(a, b, (((0,), (0,)), ((), ())), preferred_element_type=F32)


def halves(value):
    high = value.astype(BF16)
    return high, (value - high.astype(F32)).astype(BF16)


def one_minus_exp_neg(x):
    series = x * (1.0 - x * (0.5 - x * (1.0 / 6 - x * (1.0 / 24 - x * (1.0 / 120 - x / 720)))))
    return jnp.where(x < 0.25, series, 1.0 - jnp.exp(-x))


def expand(value):
    both = jnp.concatenate([value, value], axis=1)
    row, lane = iota((8, 128), 0), iota((8, 128), 1)
    parts = [
        jnp.sum(jnp.where(row == 2 * q + (lane >= 64).astype(jnp.int32), both, 0.0), axis=0, keepdims=True)
        for q in range(4)
    ]
    return jnp.concatenate(parts, axis=1)


def inclusive(a, s, backward):
    row = iota(s[0].shape, 0)
    for shift in (1, 2, 4):
        ok = row < 8 - shift if backward else row >= shift
        turn = 8 - shift if backward else shift
        pa = tuple(pltpu.roll(v, turn, 0) for v in a)
        ps = tuple(pltpu.roll(v, turn, 0) for v in s)
        na, ns = cmul(a, pa), cmul(a, ps)
        s = tuple(jnp.where(ok, n + o, o) for n, o in zip(ns, s))
        a = tuple(jnp.where(ok, n, o) for n, o in zip(na, a))
    return a, s


def exclusive(a, s, backward):
    row = iota(s[0].shape, 0)
    ok = row < 7 if backward else row >= 1
    turn = 7 if backward else 1
    ident = (1.0, 0.0)
    ea = tuple(jnp.where(ok, pltpu.roll(v, turn, 0), i) for v, i in zip(a, ident))
    es = tuple(jnp.where(ok, pltpu.roll(v, turn, 0), 0.0) for v in s)
    return ea, es


def product(g):
    for shift in (1, 2, 4):
        g = g * pltpu.roll(g, shift, 0)
    return g


def pick(value, index):
    row = iota(value.shape, 0)
    return jnp.sum(jnp.where(row == index, value, 0.0), axis=0, keepdims=True)


INPUTS = (
    ((48, 2048), BF16), ((192, 128), BF16), ((8, 192), F32), ((2, 8, 64), F32), ((2, 8, 64), F32),
    ((256, 64), F32), ((256, 64), F32), ((256, 64), F32), ((256, 64), F32), ((1, 128), F32),
    ((512, 2048), BF16), ((1, 2048), F32), ((2, 192), jnp.int32), ((1, 192), F32), ((2, 192), F32),
    ((2048, 256), BF16), ((2048, 256), BF16), ((256, 2048), BF16),
)


def kernel(*refs):
    count = len(INPUTS)
    sources, out, held = refs[:count], refs[count], refs[count + 1 : 2 * count + 1]
    (
        residual, mixer_input, log_gate, decay_rate, turn_rate, drive_real, drive_imag, read_real,
        read_imag, skip_gain, project, norm_gain, routes, group_weight, expert_weight,
        w_gate, w_linear, w_down,
    ) = held
    (
        gates, push, msg1, recv1, msg2, recv2, dec1, keep1, dec2, keep2, act_out, act_in, middle, rows, tables, taken, combine,
        swap, out1, in1, out2, xin, hidden, opp_out, fwd, right_out, left_out, sums, keep_r, keep_l, keep_o, ans, b2in, b2out, b1in,
        w_sem, small_send, small_recv, yc_send, yc_recv, z_send, z_recv, z_back, x_send, x_recv,
        o_recv, rs_send, rs_recv,
    ) = refs[2 * count + 1 :]
    sp, x = lax.axis_index("sp"), lax.axis_index("tp")
    z, yc = sp // 8, lax.rem(sp, 8)
    right, left = lax.rem(x + 1, 4), lax.rem(x + 3, 4)

    def yc_peer(k):
        other = lax.rem(yc + k, 8)
        return other, (z * 8 + other, x)

    def z_peer(k):
        other = lax.rem(z + k, 8)
        return other, (other * 8 + yc, x)

    def send(src, dst, s_sem, r_sem, device):
        pltpu.make_async_remote_copy(
            src_ref=src, dst_ref=dst, send_sem=s_sem, recv_sem=r_sem,
            device_id=device, device_id_type=MESH,
        ).start()

    def settle(ref, sem):
        pltpu.make_async_copy(ref, ref, sem).wait()

    barrier = pltpu.get_barrier_semaphore()
    for k in FAR:
        pl.semaphore_signal(barrier, inc=1, device_id=z_peer(k)[1], device_id_type=MESH)
    for k in FAR:
        pl.semaphore_signal(barrier, inc=1, device_id=yc_peer(k)[1], device_id_type=MESH)
    for k in range(1, 4):
        pl.semaphore_signal(barrier, inc=1, device_id=(sp, lax.rem(x + k, 4)), device_id_type=MESH)
    loads = [pltpu.make_async_copy(a, b, w_sem.at[n]) for n, (a, b) in enumerate(zip(sources, held))]
    first_needed = (1, 2, 3, 4, 5, 6)
    for n in first_needed:
        loads[n].start()
    for n in range(count):
        if n not in first_needed:
            loads[n].start()
    for n in first_needed:
        loads[n].wait()

    r_id, t_id = iota((192, 192), 0), iota((192, 192), 1)
    order = (t_id == lax.rem(r_id, 8) * SEGMENT + r_id // 8).astype(F32).astype(BF16)
    inputs_bf = dot(order, mixer_input[...]).astype(BF16)
    double = jnp.concatenate([inputs_bf, inputs_bf], axis=1)

    gate_rows = jnp.exp(log_gate[...])
    g1 = gate_rows.astype(BF16).astype(F32)
    g2 = (gate_rows - g1).astype(BF16).astype(F32)
    g3 = gate_rows - g1 - g2
    three = jnp.concatenate([g1, g2, g3], axis=0).astype(BF16)
    three = dot_nt(three, order).astype(BF16)
    widen = (lax.rem(iota((24, 512), 0), 8) == iota((24, 512), 1) // 64).astype(F32).astype(BF16)
    wide = dot_tn(three, widen)
    for q in range(4):
        gates[q] = wide[:, 128 * q : 128 * (q + 1)]

    step, power24, power192, power1536 = [], [], [], []
    scale = []
    for d in range(2):
        rate, turn = decay_rate[d], turn_rate[d]
        retain = jnp.exp(-rate)
        step.append((expand(retain * jnp.cos(turn)), expand(retain * jnp.sin(turn))))
        scale.append(expand(jnp.sqrt(one_minus_exp_neg(2.0 * rate))))
        p = step[d]
        for _ in range(3):
            p = cmul(p, p)
        p24 = cmul(cmul(p, p), p)
        power24.append(p24)
        p = p24
        for _ in range(3):
            p = cmul(p, p)
        power192.append(p)
        for _ in range(3):
            p = cmul(p, p)
        power1536.append(p)

    def block_diagonal(table, q):
        both = jnp.concatenate([table, table], axis=1)
        group = iota((128, 128), 0) // 16
        lane = iota((128, 128), 1)
        return jnp.where(group == 2 * q + (lane >= 64).astype(jnp.int32), both, 0.0)

    def pair(table, q):
        return jnp.concatenate([block_diagonal(table, q), block_diagonal(table, q + 1)], axis=1)

    for d in range(2):
        for part, table_ref in enumerate((drive_real, drive_imag)):
            table = table_ref[pl.ds(128 * d, 128), :]
            for q in range(0, 4, 2):
                high, low = halves(pair(table, q) * scale[d][:, 128 * q : 128 * (q + 2)])
                pushed = dot(double, jnp.concatenate([high, low], axis=0))
                push[2 * d + part, q] = pushed[:, :128]
                push[2 * d + part, q + 1] = pushed[:, 128:]

    steps = [
        [
            tuple(jnp.broadcast_to(step[d][m][:, 128 * q : 128 * (q + 1)], (8, 128)) for m in range(2))
            for q in range(4)
        ]
        for d in range(2)
    ]

    def sweep(initial, final):
        def body(j, carried):
            states, decay = carried
            new = []
            new_decay = []
            for d in range(2):
                at = pl.multiple_of((j if d == 0 else SEGMENT - 1 - j) * 8, 8)
                for q in range(4):
                    re, im = states[2 * (4 * d + q)], states[2 * (4 * d + q) + 1]
                    g = gates[q, pl.ds(at, 8), :]
                    if d == 0 and not final:
                        new_decay.append(decay[q] * g)
                    sr, si = steps[d][q]
                    nr = g * (sr * re - si * im) + push[2 * d, q, pl.ds(at, 8), :]
                    ni = g * (sr * im + si * re) + push[2 * d + 1, q, pl.ds(at, 8), :]
                    if final:
                        push[2 * d, q, pl.ds(at, 8), :] = nr
                        push[2 * d + 1, q, pl.ds(at, 8), :] = ni
                    new += [nr, ni]
            return tuple(new), tuple(new_decay)

        ones = () if final else tuple(jnp.ones((8, 128), F32) for _ in range(4))
        return lax.fori_loop(0, SEGMENT, body, (initial, ones))

    def put(msg, d, m, row):
        for q in range(4):
            msg[d, pl.ds(4 * m + q, 1), :] = row[:, 128 * q : 128 * (q + 1)]


    zeros = tuple(jnp.zeros((8, 128), F32) for _ in range(16))
    ends, decay = sweep(zeros, False)
    decay = jnp.concatenate(decay, axis=1)
    enter = []
    for d in range(2):
        s = tuple(jnp.concatenate([ends[2 * (4 * d + q) + m] for q in range(4)], axis=1) for m in range(2))
        a = tuple(decay * p for p in power24[d])
        a, s = inclusive(a, s, d == 1)
        enter.append(exclusive(a, s, d == 1))
        last = 0 if d == 1 else 7
        for m in range(2):
            put(msg1, d, m, s[m][last : last + 1, :])
    dec1[0] = product(decay)[0:1, :]

    pl.semaphore_wait(barrier, 17)

    def gathered(recv, slab, first_row):
        return jnp.concatenate([recv[:, slab, first_row + q, :] for q in range(4)], axis=1)

    def combined(recv, kept, me, powers, masked):
        decays = kept[:, 0, :]
        row = iota((8, 512), 0)
        found = []
        for d in range(2):
            s = tuple(gathered(recv, d, 4 * m) for m in range(2))
            if masked:
                used = row > me if d == 1 else row < me
                s = tuple(jnp.where(used, v, 0.0) for v in s)
            a = tuple(decays * p for p in powers[d])
            a, s = inclusive(a, s, d == 1)
            ea, es = exclusive(a, s, d == 1)
            last = 0 if d == 1 else 7
            found.append(
                (
                    tuple(pick(v, me) for v in ea),
                    tuple(pick(v, me) for v in es),
                    tuple(v[last : last + 1, :] for v in s),
                )
            )
        return found, decays

    for k in FAR:
        send(msg1, recv1.at[yc], small_send.at[0], small_recv.at[0], yc_peer(k)[1])
        send(dec1.at[0], keep1.at[yc], small_send.at[3], small_recv.at[3], yc_peer(k)[1])
    recv1[pl.ds(yc, 1)] = msg1[...][None]
    keep1[pl.ds(yc, 1)] = dec1[...]

    for n in (7, 8, 12, 13, 14):
        loads[n].wait()
    for index in range(4):
        d, part = divmod(index, 2)
        table = (read_real, read_imag)[part][pl.ds(128 * d, 128), :]
        table = table if part == 0 else -table
        for q in range(0, 4, 2):
            tables[index, q // 2] = jnp.concatenate(halves(pair(table, q)), axis=0)
    chosen = routes[...].astype(F32)
    weights = expert_weight[...]
    mixing = group_weight[...] * weights / jnp.sum(weights, axis=0, keepdims=True)
    own = iota((192, 128), 0) == 48 * x + iota((192, 128), 1)
    own = (own & (iota((192, 128), 1) < 48)).astype(F32)
    chosen = jnp.dot(chosen, own, precision=lax.Precision.HIGHEST, preferred_element_type=F32)
    mixing = jnp.dot(mixing, own, precision=lax.Precision.HIGHEST, preferred_element_type=F32)
    slot, lane = iota((128, 128), 0), iota((128, 128), 1)
    place = lax.rem(slot, 16) // 2
    offset = jnp.zeros_like(place)
    for i in range(1, 8):
        offset = jnp.where(place == i, ORDER[i], offset)
    expert = (lax.rem(z + offset, 8) * 8 + slot // 16).astype(F32)
    first = (chosen[0:1, :] == expert) & (lane < 48)
    second = (chosen[1:2, :] == expert) & (lane < 48)
    match = jnp.where(first | second, 1.0, 0.0)
    earlier = (slot < lane).astype(F32).astype(BF16)
    rank = dot(match.astype(BF16), earlier)
    mine = jnp.where(rank == lax.rem(slot, 2).astype(F32), match, 0.0)
    taken[...] = mine.astype(BF16)
    mine = mine * jnp.where(first, mixing[0:1, :], mixing[1:2, :])
    combine[0], combine[1] = halves(mine.T)
    swapped = place * 16 + slot // 16 * 2 + lax.rem(slot, 2)
    swap[...] = (lane == swapped).astype(F32).astype(BF16)
    rows[pl.ds(48, 80), :] = jnp.zeros((80, CHUNKS * WIDE), BF16)

    settle(recv1.at[pl.ds(0, 7)], small_recv.at[0])
    settle(keep1.at[pl.ds(0, 7)], small_recv.at[3])
    found1, decays = combined(recv1, keep1, yc, power192, False)
    for d in range(2):
        for m in range(2):
            put(msg2, d, m, found1[d][2][m])
    dec2[0] = product(decays)[0:1, :]
    for k in FAR:
        other, device = z_peer(k)
        part = jnp.where(other > z, 0, 1)
        send(msg2.at[part], recv2.at[z, part], small_send.at[1], small_recv.at[1], device)
        send(dec2.at[0], keep2.at[z], small_send.at[4], small_recv.at[4], device)
    recv2[pl.ds(z, 1)] = msg2[...][None]
    keep2[pl.ds(z, 1)] = dec2[...]
    settle(recv2.at[pl.ds(0, 7), 0], small_recv.at[1])
    settle(keep2.at[pl.ds(0, 7)], small_recv.at[4])
    found2, _ = combined(recv2, keep2, z, power1536, True)
    initial = []
    for d in range(2):
        pa, ps, _ = found1[d]
        carry = cmul(pa, found2[d][1])
        carry = tuple(c + p for c, p in zip(carry, ps))
        ea, es = enter[d]
        begin = cmul(ea, carry)
        begin = tuple(f + e for f, e in zip(begin, es))
        for q in range(4):
            initial += [f[:, 128 * q : 128 * (q + 1)] for f in begin]
    sweep(tuple(initial), True)

    loads[9].wait()
    readout = skip_gain[...] * inputs_bf.astype(F32)
    both = jnp.zeros((192, 256), F32)
    for index in range(4):
        for q in range(0, 4, 2):
            s_high, s_low = halves(jnp.concatenate([push[index, q], push[index, q + 1]], axis=1))
            both = both + dot_nt(s_high, tables[index, q // 2])
            readout = readout + dot_nt(s_low, tables[index, q // 2, pl.ds(0, 128), :])
    readout = readout + both[:, :128] + both[:, 128:]
    inner = 0.7978845608028654 * (readout + 0.044715 * readout * readout * readout)
    activated = (0.5 * readout * (1.0 + jnp.tanh(inner))).astype(BF16)
    r_id, t_id = iota((192, 192), 0), iota((192, 192), 1)
    order_back = (r_id == lax.rem(t_id, 8) * SEGMENT + t_id // 8).astype(F32).astype(BF16)
    activated = dot(order_back, activated).astype(BF16)
    act_out[...] = activated.reshape(4, 48, 128)
    for k in (2, 1, 3):
        other = lax.rem(x + k, 4)
        send(act_out.at[other], act_in.at[x], small_send.at[2], small_recv.at[2], (sp, other))
    act_in[pl.ds(x, 1)] = act_out[pl.ds(x, 1)]

    for n in (0, 10, 11):
        loads[n].wait()
    settle(act_in.at[pl.ds(0, 3)], small_recv.at[2])
    channels = jnp.concatenate([act_in[m] for m in range(4)], axis=1)
    total = jnp.zeros((48, 1), F32)
    for c in range(CHUNKS):
        cols = pl.ds(WIDE * c, WIDE)
        v = deep_alpha * residual[:, cols].astype(F32) + dot(channels, project[:, cols])
        middle[:, cols] = v
        total = total + jnp.sum(v, axis=1, keepdims=True)
    mean = total / (CHUNKS * WIDE)
    total = jnp.zeros((48, 1), F32)
    for c in range(CHUNKS):
        center = middle[:, pl.ds(WIDE * c, WIDE)] - mean
        total = total + jnp.sum(center * center, axis=1, keepdims=True)
    factor = lax.rsqrt(total / (CHUNKS * WIDE) + norm_epsilon)
    for c in range(CHUNKS):
        cols = pl.ds(WIDE * c, WIDE)
        v = (middle[:, cols] - mean) * factor * norm_gain[:, cols]
        middle[:, cols] = v
        rows[pl.ds(0, 48), cols] = v.astype(BF16)
        out1[:, :, cols] = dot(taken[...], rows[:, cols]).astype(BF16).reshape(8, 16, WIDE)
        for k in FAR:
            other, device = yc_peer(k)
            send(out1.at[other, :, cols], in1.at[yc, :, cols], yc_send.at[0], yc_recv.at[0, c], device)
        in1[pl.ds(yc, 1), :, cols] = out1[pl.ds(yc, 1), :, cols]

    def side(h):
        return pl.ds(HALF * h, HALF)

    def start_z(i, h, cols):
        to = LANDS[i]
        send(
            out2.at[i, :, cols], xin.at[0, to, :, cols], z_send.at[0], z_recv.at[to, h],
            z_peer(ORDER[i])[1],
        )

    def spread(i, h, cols):
        block = xin.at[0, i, :, cols]
        rest = o_recv.at[i // 4]
        send(block, xin.at[1, i, :, cols], x_send.at[0], rest if h else x_recv.at[0, i], (sp, right))
        send(block, xin.at[2, i, :, cols], x_send.at[1], x_recv.at[1, i] if h else rest, (sp, left))

    def pass_on(i, h):
        block = xin.at[1 + h, i, :, side(h)]
        settle(block, x_recv.at[h, i])
        send(block, xin.at[3, i, :, side(h)], x_send.at[2 + h], o_recv.at[i // 4], (sp, (right, left)[h]))

    for c in range(CHUNKS):
        cols = pl.ds(WIDE * c, WIDE)
        settle(in1.at[pl.ds(0, 7), :, cols], yc_recv.at[0, c])
        moved = dot(swap[...], in1[:, :, cols].reshape(128, WIDE)).astype(BF16)
        out2[:, :, cols] = moved.reshape(8, 16, WIDE)
        xin[0, 0, :, cols] = moved[0:16, :]
        for i in range(1, 4):
            start_z(i, c // 2, cols)
        spread(0, c // 2, cols)
    for i in range(4, 5):
        for h in range(2):
            start_z(i, h, side(h))

    def multiply(g):
        settle(xin.at[pl.ds(2, 2), pl.ds(4 * g, 4)], o_recv.at[g])
        block = xin[:, pl.ds(4 * g, 4)].reshape(256, 2048)
        gate = dot(block, w_gate[...])
        linear = dot(block, w_linear[...])
        hidden[g] = (gate / (1.0 + jnp.exp(-gate)) * linear).astype(BF16)

    low, high = pl.ds(0, 2), pl.ds(2, 2)

    def start_sums(g, c):
        cols = pl.ds(WIDE * c, WIDE)
        part = dot(hidden[g], w_down[:, cols]).reshape(4, 4, 16, WIDE)
        opp_out[g, :, :, cols] = part[3].astype(BF16)
        send(opp_out.at[g, low, :, cols], fwd.at[0, g, :, :, cols], rs_send.at[0], rs_recv.at[0, g, c], (sp, right))
        send(opp_out.at[g, high, :, cols], fwd.at[1, g, :, :, cols], rs_send.at[1], rs_recv.at[2, g, c], (sp, left))
        right_out[g, high, :, cols] = part[2, 2:4].astype(BF16)
        keep_r[g, :, :, cols] = part[2, 0:2]
        send(right_out.at[g, high, :, cols], sums.at[0, g, high, :, cols], rs_send.at[2], rs_recv.at[1, g, c], (sp, right))
        left_out[g, low, :, cols] = part[1, 0:2].astype(BF16)
        keep_l[g, :, :, cols] = part[1, 2:4]
        send(left_out.at[g, low, :, cols], sums.at[1, g, low, :, cols], rs_send.at[3], rs_recv.at[1, g, c], (sp, left))
        keep_o[g, :, :, cols] = part[0]

    def add_on(g, c):
        cols = pl.ds(WIDE * c, WIDE)
        settle(fwd.at[0, g, :, :, cols], rs_recv.at[0, g, c])
        right_out[g, low, :, cols] = (keep_r[g, :, :, cols] + fwd[0, g, :, :, cols].astype(F32)).astype(BF16)
        send(right_out.at[g, low, :, cols], sums.at[0, g, low, :, cols], rs_send.at[2], rs_recv.at[1, g, c], (sp, right))
        settle(fwd.at[1, g, :, :, cols], rs_recv.at[2, g, c])
        left_out[g, high, :, cols] = (keep_l[g, :, :, cols] + fwd[1, g, :, :, cols].astype(F32)).astype(BF16)
        send(left_out.at[g, high, :, cols], sums.at[1, g, high, :, cols], rs_send.at[3], rs_recv.at[1, g, c], (sp, left))

    def finish_sums(g, c):
        cols = pl.ds(WIDE * c, WIDE)
        settle(sums.at[:, g, :, :, cols], rs_recv.at[1, g, c])
        part = keep_o[g, :, :, cols] + sums[0, g, :, :, cols].astype(F32) + sums[1, g, :, :, cols].astype(F32)
        ans[pl.ds(4 * g, 4), :, cols] = part.astype(BF16)
        for i in range(4 * g, 4 * g + 4):
            if i == 0:
                b2in[0, :, cols] = ans[0, :, cols]
                continue
            send(ans.at[i, :, cols], b2in.at[LANDS[i], :, cols], z_send.at[1], z_back.at[c], z_peer(ORDER[i])[1])

    def go_home(c):
        cols = pl.ds(WIDE * c, WIDE)
        settle(b2in.at[pl.ds(0, 7), :, cols], z_back.at[c])
        moved = dot(swap[...], b2in[:, :, cols].reshape(128, WIDE)).astype(BF16)
        b2out[:, :, cols] = moved.reshape(8, 16, WIDE)
        for k in FAR:
            other, device = yc_peer(k)
            send(b2out.at[other, :, cols], b1in.at[yc, :, cols], yc_send.at[1], yc_recv.at[1, c], device)
        b1in[pl.ds(yc, 1), :, cols] = b2out[pl.ds(yc, 1), :, cols]

    for i in range(1, 8):
        for h in range(2):
            settle(xin.at[0, i, :, side(h)], z_recv.at[i, h])
            spread(i, h, side(h))
            if i == 1:
                pass_on(0, h)
        for later in {1: (5, 6), 2: (7,)}.get(i, ()):
            for h in range(2):
                start_z(later, h, side(h))
        if i > 2:
            pass_on(i - 2, 0)
            pass_on(i - 2, 1)
        if i == 1:
            for n in (15, 16, 17):
                loads[n].wait()
    multiply(0)
    pass_on(6, 0)
    pass_on(6, 1)
    pass_on(7, 0)
    pass_on(7, 1)
    start_sums(0, 0)
    start_sums(0, 1)
    multiply(1)
    start_sums(1, 0)
    start_sums(1, 1)
    add_on(0, 0)
    add_on(0, 1)
    start_sums(1, 2)
    add_on(1, 0)
    start_sums(1, 3)
    add_on(1, 1)
    start_sums(0, 2)
    start_sums(0, 3)
    finish_sums(0, 0)
    add_on(1, 2)
    finish_sums(0, 1)
    finish_sums(1, 0)
    add_on(1, 3)
    finish_sums(1, 1)
    add_on(0, 2)
    finish_sums(1, 2)
    add_on(0, 3)
    finish_sums(1, 3)
    finish_sums(0, 2)
    finish_sums(0, 3)
    for c in range(CHUNKS):
        go_home(c)

    total = jnp.zeros((48, 1), F32)
    for c in range(CHUNKS):
        cols = pl.ds(WIDE * c, WIDE)
        settle(b1in.at[pl.ds(0, 7), :, cols], yc_recv.at[1, c])
        back = b1in[:, :, cols].reshape(128, WIDE)
        routed = dot(combine[0, pl.ds(0, 48), :], back) + dot(combine[1, pl.ds(0, 48), :], back)
        v = deep_alpha * middle[:, cols] + routed
        middle[:, cols] = v
        total = total + jnp.sum(v, axis=1, keepdims=True)
    mean = total / (CHUNKS * WIDE)
    total = jnp.zeros((48, 1), F32)
    for c in range(CHUNKS):
        center = middle[:, pl.ds(WIDE * c, WIDE)] - mean
        total = total + jnp.sum(center * center, axis=1, keepdims=True)
    factor = lax.rsqrt(total / (CHUNKS * WIDE) + norm_epsilon)
    for c in range(CHUNKS):
        cols = pl.ds(WIDE * c, WIDE)
        out[:, cols] = (middle[:, cols] - mean) * factor

    settle(recv1.at[pl.ds(0, 7)], small_send.at[0])
    settle(recv2.at[pl.ds(0, 7), 0], small_send.at[1])
    settle(keep1.at[pl.ds(0, 7)], small_send.at[3])
    settle(keep2.at[pl.ds(0, 7)], small_send.at[4])
    settle(act_in.at[pl.ds(0, 3)], small_send.at[2])
    for index in range(2):
        settle(out1.at[pl.ds(0, 7)], yc_send.at[index])
        settle(out2.at[pl.ds(0, 7)], z_send.at[index])
        settle(xin.at[0], x_send.at[index])
        settle(xin.at[0, pl.ds(0, 4)], x_send.at[2 + index])
        settle(fwd.at[0], rs_send.at[index])
        settle(sums.at[0], rs_send.at[2 + index])


def on_device(
    residual, mixer_input, log_gate, decay_rate, turn_rate, drive_real, drive_imaginary, read_real,
    read_imaginary, skip_gain, project_weight, norm_gain, final_gain, routes, group_weight,
    expert_weight, gate_weight, linear_weight, down_weight,
):
    dma = pltpu.SemaphoreType.DMA
    slab = pltpu.VMEM((8, 16, 2048), BF16)
    groups = pltpu.VMEM((2, 4, 16, 2048), BF16)
    normed = pl.pallas_call(
        kernel,
        out_shape=jax.ShapeDtypeStruct((48, 2048), F32),
        in_specs=[pl.BlockSpec(memory_space=pl.ANY)] * len(INPUTS),
        out_specs=pl.BlockSpec(memory_space=pltpu.VMEM),
        scratch_shapes=[pltpu.VMEM(shape, dtype) for shape, dtype in INPUTS]
        + [
            pltpu.VMEM((4, 192, 128), F32),
            pltpu.VMEM((4, 4, 192, 128), F32),
            pltpu.VMEM((2, 8, 128), F32),
            pltpu.VMEM((8, 2, 8, 128), F32),
            pltpu.VMEM((2, 8, 128), F32),
            pltpu.VMEM((8, 2, 8, 128), F32),
            pltpu.VMEM((1, 1, 512), F32),
            pltpu.VMEM((8, 1, 512), F32),
            pltpu.VMEM((1, 1, 512), F32),
            pltpu.VMEM((8, 1, 512), F32),
            pltpu.VMEM((4, 48, 128), BF16),
            pltpu.VMEM((4, 48, 128), BF16),
            pltpu.VMEM((48, 2048), F32),
            pltpu.VMEM((128, 2048), BF16),
            pltpu.VMEM((4, 2, 256, 256), BF16),
            pltpu.VMEM((128, 128), BF16),
            pltpu.VMEM((2, 128, 128), BF16),
            pltpu.VMEM((128, 128), BF16),
            slab, slab, slab,
            pltpu.VMEM((4, 8, 16, 2048), BF16),
            pltpu.VMEM((2, 256, 256), BF16),
            groups,
            pltpu.VMEM((2, 2, 2, 16, 2048), BF16),
            groups, groups,
            pltpu.VMEM((2, 2, 4, 16, 2048), BF16),
            pltpu.VMEM((2, 2, 16, 2048), F32),
            pltpu.VMEM((2, 2, 16, 2048), F32),
            pltpu.VMEM((2, 4, 16, 2048), F32),
            slab, slab, slab, slab,
            dma((len(INPUTS),)), dma((5,)), dma((5,)),
            dma((2,)), dma((2, CHUNKS)), dma((2,)), dma((8, 2)), dma((CHUNKS,)),
            dma((4,)), dma((2, 8)), dma((2,)),
            dma((4,)), dma((3, 2, CHUNKS)),
        ],
        compiler_params=pltpu.CompilerParams(
            collective_id=0, has_side_effects=True, vmem_limit_bytes=40 * 1024 * 1024
        ),
        name="layer",
    )(*(pltpu.with_memory_space_constraint(v, pltpu.HBM) for v in (
        residual, mixer_input, log_gate.T, decay_rate, turn_rate,
        drive_real.reshape(256, 64), drive_imaginary.reshape(256, 64),
        read_real.reshape(256, 64), read_imaginary.reshape(256, 64),
        skip_gain.reshape(1, 128), project_weight, norm_gain.reshape(1, 2048),
        routes.T, group_weight.reshape(1, 192), expert_weight.T,
        gate_weight[0], linear_weight[0], down_weight[0],
    )))
    return (normed * final_gain).astype(BF16)


def solution(mesh):
    placed = (
        P(("sp", "tp"), None),
        P("sp", "tp"),
        P("sp", "tp"),
        P(None, "tp", None),
        P(None, "tp", None),
        P(None, "tp", None, None),
        P(None, "tp", None, None),
        P(None, "tp", None, None),
        P(None, "tp", None, None),
        P("tp"),
        P(),
        P(),
        P(),
        P("sp", None),
        P("sp"),
        P("sp", None),
        P("sp", None, "tp"),
        P("sp", None, "tp"),
        P("sp", "tp", None),
    )
    return jax.shard_map(
        on_device, mesh=mesh, in_specs=placed, out_specs=P(("sp", "tp"), None), check_vma=False
    )
```

```python
import jax
import jax.numpy as jnp
from jax import lax
from jax.experimental import pallas as pl
from jax.experimental.pallas import tpu as pltpu
from jax.sharding import PartitionSpec as P

MESH = pl.DeviceIdType.MESH
F32 = jnp.float32
BF16 = jnp.bfloat16
deep_alpha = 2.0**0.25
norm_epsilon = 1e-05
SEGMENT = 24
CHUNKS = 4
WIDE = 512
HALF = 1024
FAR = (4, 3, 5, 2, 6, 1, 7)
ORDER = (0, 1, 7, 2, 6, 3, 5, 4)
LANDS = tuple(ORDER.index((8 - k) % 8) for k in ORDER)


def iota(shape, dim):
    return lax.broadcasted_iota(jnp.int32, shape, dim)


def cmul(a, b):
    return (a[0] * b[0] - a[1] * b[1], a[0] * b[1] + a[1] * b[0])


def dot(a, b):
    return jnp.dot(a, b, preferred_element_type=F32)


def dot_nt(a, b):
    return lax.dot_general(a, b, (((1,), (1,)), ((), ())), preferred_element_type=F32)


def dot_tn(a, b):
    return lax.dot_general(a, b, (((0,), (0,)), ((), ())), preferred_element_type=F32)


def halves(value):
    high = value.astype(BF16)
    return high, (value - high.astype(F32)).astype(BF16)


def one_minus_exp_neg(x):
    series = x * (1.0 - x * (0.5 - x * (1.0 / 6 - x * (1.0 / 24 - x * (1.0 / 120 - x / 720)))))
    return jnp.where(x < 0.25, series, 1.0 - jnp.exp(-x))


def expand(value):
    both = jnp.concatenate([value, value], axis=1)
    row, lane = iota((8, 128), 0), iota((8, 128), 1)
    parts = [
        jnp.sum(jnp.where(row == 2 * q + (lane >= 64).astype(jnp.int32), both, 0.0), axis=0, keepdims=True)
        for q in range(4)
    ]
    return jnp.concatenate(parts, axis=1)


def inclusive(a, s, backward):
    row = iota(s[0].shape, 0)
    for shift in (1, 2, 4):
        ok = row < 8 - shift if backward else row >= shift
        turn = 8 - shift if backward else shift
        pa = tuple(pltpu.roll(v, turn, 0) for v in a)
        ps = tuple(pltpu.roll(v, turn, 0) for v in s)
        na, ns = cmul(a, pa), cmul(a, ps)
        s = tuple(jnp.where(ok, n + o, o) for n, o in zip(ns, s))
        a = tuple(jnp.where(ok, n, o) for n, o in zip(na, a))
    return a, s


def exclusive(a, s, backward):
    row = iota(s[0].shape, 0)
    ok = row < 7 if backward else row >= 1
    turn = 7 if backward else 1
    ident = (1.0, 0.0)
    ea = tuple(jnp.where(ok, pltpu.roll(v, turn, 0), i) for v, i in zip(a, ident))
    es = tuple(jnp.where(ok, pltpu.roll(v, turn, 0), 0.0) for v in s)
    return ea, es


def product(g):
    for shift in (1, 2, 4):
        g = g * pltpu.roll(g, shift, 0)
    return g


def pick(value, index):
    row = iota(value.shape, 0)
    return jnp.sum(jnp.where(row == index, value, 0.0), axis=0, keepdims=True)


INPUTS = (
    ((48, 2048), BF16), ((192, 128), BF16), ((8, 192), F32), ((2, 8, 64), F32), ((2, 8, 64), F32),
    ((256, 64), F32), ((256, 64), F32), ((256, 64), F32), ((256, 64), F32), ((1, 128), F32),
    ((512, 2048), BF16), ((1, 2048), F32), ((2, 192), jnp.int32), ((1, 192), F32), ((2, 192), F32),
    ((2048, 256), BF16), ((2048, 256), BF16), ((256, 2048), BF16),
)


def kernel(*refs):
    count = len(INPUTS)
    sources, out, held = refs[:count], refs[count], refs[count + 1 : 2 * count + 1]
    (
        residual, mixer_input, log_gate, decay_rate, turn_rate, drive_real, drive_imag, read_real,
        read_imag, skip_gain, project, norm_gain, routes, group_weight, expert_weight,
        w_gate, w_linear, w_down,
    ) = held
    (
        gates, push, msg1, recv1, msg2, recv2, dec1, keep1, dec2, keep2, act_out, act_in, middle, rows, tables, taken, combine,
        swap, out1, in1, out2, xin, hidden, opp_out, fwd, right_out, left_out, sums, keep_r, keep_l, keep_o, ans, b2in, b2out, b1in,
        w_sem, small_send, small_recv, yc_send, yc_recv, z_send, z_recv, z_back, x_send, x_recv,
        o_recv, rs_send, rs_recv,
    ) = refs[2 * count + 1 :]
    sp, x = lax.axis_index("sp"), lax.axis_index("tp")
    z, yc = sp // 8, lax.rem(sp, 8)
    right, left = lax.rem(x + 1, 4), lax.rem(x + 3, 4)

    def yc_peer(k):
        other = lax.rem(yc + k, 8)
        return other, (z * 8 + other, x)

    def z_peer(k):
        other = lax.rem(z + k, 8)
        return other, (other * 8 + yc, x)

    def send(src, dst, s_sem, r_sem, device):
        pltpu.make_async_remote_copy(
            src_ref=src, dst_ref=dst, send_sem=s_sem, recv_sem=r_sem,
            device_id=device, device_id_type=MESH,
        ).start()

    def settle(ref, sem):
        pltpu.make_async_copy(ref, ref, sem).wait()

    barrier = pltpu.get_barrier_semaphore()
    for k in FAR:
        pl.semaphore_signal(barrier, inc=1, device_id=z_peer(k)[1], device_id_type=MESH)
    for k in FAR:
        pl.semaphore_signal(barrier, inc=1, device_id=yc_peer(k)[1], device_id_type=MESH)
    for k in range(1, 4):
        pl.semaphore_signal(barrier, inc=1, device_id=(sp, lax.rem(x + k, 4)), device_id_type=MESH)
    loads = [pltpu.make_async_copy(a, b, w_sem.at[n]) for n, (a, b) in enumerate(zip(sources, held))]
    first_needed = (1, 2, 3, 4, 5, 6)
    for n in first_needed:
        loads[n].start()
    for n in range(count):
        if n not in first_needed:
            loads[n].start()
    for n in first_needed:
        loads[n].wait()

    r_id, t_id = iota((192, 192), 0), iota((192, 192), 1)
    order = (t_id == lax.rem(r_id, 8) * SEGMENT + r_id // 8).astype(F32).astype(BF16)
    inputs_bf = dot(order, mixer_input[...]).astype(BF16)
    double = jnp.concatenate([inputs_bf, inputs_bf], axis=1)

    gate_rows = jnp.exp(log_gate[...])
    g1 = gate_rows.astype(BF16).astype(F32)
    g2 = (gate_rows - g1).astype(BF16).astype(F32)
    g3 = gate_rows - g1 - g2
    three = jnp.concatenate([g1, g2, g3], axis=0).astype(BF16)
    three = dot_nt(three, order).astype(BF16)
    widen = (lax.rem(iota((24, 512), 0), 8) == iota((24, 512), 1) // 64).astype(F32).astype(BF16)
    wide = dot_tn(three, widen)
    for q in range(4):
        gates[q] = wide[:, 128 * q : 128 * (q + 1)]

    step, power24, power192, power1536 = [], [], [], []
    scale = []
    for d in range(2):
        rate, turn = decay_rate[d], turn_rate[d]
        retain = jnp.exp(-rate)
        step.append((expand(retain * jnp.cos(turn)), expand(retain * jnp.sin(turn))))
        scale.append(expand(jnp.sqrt(one_minus_exp_neg(2.0 * rate))))
        p = step[d]
        for _ in range(3):
            p = cmul(p, p)
        p24 = cmul(cmul(p, p), p)
        power24.append(p24)
        p = p24
        for _ in range(3):
            p = cmul(p, p)
        power192.append(p)
        for _ in range(3):
            p = cmul(p, p)
        power1536.append(p)

    def block_diagonal(table, q):
        both = jnp.concatenate([table, table], axis=1)
        group = iota((128, 128), 0) // 16
        lane = iota((128, 128), 1)
        return jnp.where(group == 2 * q + (lane >= 64).astype(jnp.int32), both, 0.0)

    def pair(table, q):
        return jnp.concatenate([block_diagonal(table, q), block_diagonal(table, q + 1)], axis=1)

    for d in range(2):
        for part, table_ref in enumerate((drive_real, drive_imag)):
            table = table_ref[pl.ds(128 * d, 128), :]
            for q in range(0, 4, 2):
                high, low = halves(pair(table, q) * scale[d][:, 128 * q : 128 * (q + 2)])
                pushed = dot(double, jnp.concatenate([high, low], axis=0))
                push[2 * d + part, q] = pushed[:, :128]
                push[2 * d + part, q + 1] = pushed[:, 128:]

    steps = [
        [
            tuple(jnp.broadcast_to(step[d][m][:, 128 * q : 128 * (q + 1)], (8, 128)) for m in range(2))
            for q in range(4)
        ]
        for d in range(2)
    ]

    def sweep(initial, final):
        def body(j, carried):
            states, decay = carried
            new = []
            new_decay = []
            for d in range(2):
                at = pl.multiple_of((j if d == 0 else SEGMENT - 1 - j) * 8, 8)
                for q in range(4):
                    re, im = states[2 * (4 * d + q)], states[2 * (4 * d + q) + 1]
                    g = gates[q, pl.ds(at, 8), :]
                    if d == 0 and not final:
                        new_decay.append(decay[q] * g)
                    sr, si = steps[d][q]
                    nr = g * (sr * re - si * im) + push[2 * d, q, pl.ds(at, 8), :]
                    ni = g * (sr * im + si * re) + push[2 * d + 1, q, pl.ds(at, 8), :]
                    if final:
                        push[2 * d, q, pl.ds(at, 8), :] = nr
                        push[2 * d + 1, q, pl.ds(at, 8), :] = ni
                    new += [nr, ni]
            return tuple(new), tuple(new_decay)

        ones = () if final else tuple(jnp.ones((8, 128), F32) for _ in range(4))
        return lax.fori_loop(0, SEGMENT, body, (initial, ones))

    def put(msg, d, m, row):
        for q in range(4):
            msg[d, pl.ds(4 * m + q, 1), :] = row[:, 128 * q : 128 * (q + 1)]


    zeros = tuple(jnp.zeros((8, 128), F32) for _ in range(16))
    ends, decay = sweep(zeros, False)
    decay = jnp.concatenate(decay, axis=1)
    enter = []
    for d in range(2):
        s = tuple(jnp.concatenate([ends[2 * (4 * d + q) + m] for q in range(4)], axis=1) for m in range(2))
        a = tuple(decay * p for p in power24[d])
        a, s = inclusive(a, s, d == 1)
        enter.append(exclusive(a, s, d == 1))
        last = 0 if d == 1 else 7
        for m in range(2):
            put(msg1, d, m, s[m][last : last + 1, :])
    dec1[0] = product(decay)[0:1, :]

    pl.semaphore_wait(barrier, 17)

    def gathered(recv, slab, first_row):
        return jnp.concatenate([recv[:, slab, first_row + q, :] for q in range(4)], axis=1)

    def combined(recv, kept, me, powers, masked):
        decays = kept[:, 0, :]
        row = iota((8, 512), 0)
        found = []
        for d in range(2):
            s = tuple(gathered(recv, d, 4 * m) for m in range(2))
            if masked:
                used = row > me if d == 1 else row < me
                s = tuple(jnp.where(used, v, 0.0) for v in s)
            a = tuple(decays * p for p in powers[d])
            a, s = inclusive(a, s, d == 1)
            ea, es = exclusive(a, s, d == 1)
            last = 0 if d == 1 else 7
            found.append(
                (
                    tuple(pick(v, me) for v in ea),
                    tuple(pick(v, me) for v in es),
                    tuple(v[last : last + 1, :] for v in s),
                )
            )
        return found, decays

    for k in FAR:
        send(msg1, recv1.at[yc], small_send.at[0], small_recv.at[0], yc_peer(k)[1])
        send(dec1.at[0], keep1.at[yc], small_send.at[3], small_recv.at[3], yc_peer(k)[1])
    recv1[pl.ds(yc, 1)] = msg1[...][None]
    keep1[pl.ds(yc, 1)] = dec1[...]

    for n in (7, 8, 12, 13, 14):
        loads[n].wait()
    for index in range(4):
        d, part = divmod(index, 2)
        table = (read_real, read_imag)[part][pl.ds(128 * d, 128), :]
        table = table if part == 0 else -table
        for q in range(0, 4, 2):
            tables[index, q // 2] = jnp.concatenate(halves(pair(table, q)), axis=0)
    chosen = routes[...].astype(F32)
    weights = expert_weight[...]
    mixing = group_weight[...] * weights / jnp.sum(weights, axis=0, keepdims=True)
    own = iota((192, 128), 0) == 48 * x + iota((192, 128), 1)
    own = (own & (iota((192, 128), 1) < 48)).astype(F32)
    chosen = jnp.dot(chosen, own, precision=lax.Precision.HIGHEST, preferred_element_type=F32)
    mixing = jnp.dot(mixing, own, precision=lax.Precision.HIGHEST, preferred_element_type=F32)
    slot, lane = iota((128, 128), 0), iota((128, 128), 1)
    place = lax.rem(slot, 16) // 2
    offset = jnp.zeros_like(place)
    for i in range(1, 8):
        offset = jnp.where(place == i, ORDER[i], offset)
    expert = (lax.rem(z + offset, 8) * 8 + slot // 16).astype(F32)
    first = (chosen[0:1, :] == expert) & (lane < 48)
    second = (chosen[1:2, :] == expert) & (lane < 48)
    match = jnp.where(first | second, 1.0, 0.0)
    earlier = (slot < lane).astype(F32).astype(BF16)
    rank = dot(match.astype(BF16), earlier)
    mine = jnp.where(rank == lax.rem(slot, 2).astype(F32), match, 0.0)
    taken[...] = mine.astype(BF16)
    mine = mine * jnp.where(first, mixing[0:1, :], mixing[1:2, :])
    combine[0], combine[1] = halves(mine.T)
    swapped = place * 16 + slot // 16 * 2 + lax.rem(slot, 2)
    swap[...] = (lane == swapped).astype(F32).astype(BF16)
    rows[pl.ds(48, 80), :] = jnp.zeros((80, CHUNKS * WIDE), BF16)

    settle(recv1.at[pl.ds(0, 7)], small_recv.at[0])
    settle(keep1.at[pl.ds(0, 7)], small_recv.at[3])
    found1, decays = combined(recv1, keep1, yc, power192, False)
    for d in range(2):
        for m in range(2):
            put(msg2, d, m, found1[d][2][m])
    dec2[0] = product(decays)[0:1, :]
    for k in FAR:
        other, device = z_peer(k)
        part = jnp.where(other > z, 0, 1)
        send(msg2.at[part], recv2.at[z, part], small_send.at[1], small_recv.at[1], device)
        send(dec2.at[0], keep2.at[z], small_send.at[4], small_recv.at[4], device)
    recv2[pl.ds(z, 1)] = msg2[...][None]
    keep2[pl.ds(z, 1)] = dec2[...]
    settle(recv2.at[pl.ds(0, 7), 0], small_recv.at[1])
    settle(keep2.at[pl.ds(0, 7)], small_recv.at[4])
    found2, _ = combined(recv2, keep2, z, power1536, True)
    initial = []
    for d in range(2):
        pa, ps, _ = found1[d]
        carry = cmul(pa, found2[d][1])
        carry = tuple(c + p for c, p in zip(carry, ps))
        ea, es = enter[d]
        begin = cmul(ea, carry)
        begin = tuple(f + e for f, e in zip(begin, es))
        for q in range(4):
            initial += [f[:, 128 * q : 128 * (q + 1)] for f in begin]
    sweep(tuple(initial), True)

    loads[9].wait()
    readout = skip_gain[...] * inputs_bf.astype(F32)
    both = jnp.zeros((192, 256), F32)
    for index in range(4):
        for q in range(0, 4, 2):
            s_high, s_low = halves(jnp.concatenate([push[index, q], push[index, q + 1]], axis=1))
            both = both + dot_nt(s_high, tables[index, q // 2])
            readout = readout + dot_nt(s_low, tables[index, q // 2, pl.ds(0, 128), :])
    readout = readout + both[:, :128] + both[:, 128:]
    inner = 0.7978845608028654 * (readout + 0.044715 * readout * readout * readout)
    activated = (0.5 * readout * (1.0 + jnp.tanh(inner))).astype(BF16)
    r_id, t_id = iota((192, 192), 0), iota((192, 192), 1)
    order_back = (r_id == lax.rem(t_id, 8) * SEGMENT + t_id // 8).astype(F32).astype(BF16)
    activated = dot(order_back, activated).astype(BF16)
    act_out[...] = activated.reshape(4, 48, 128)
    for k in (2, 1, 3):
        other = lax.rem(x + k, 4)
        send(act_out.at[other], act_in.at[x], small_send.at[2], small_recv.at[2], (sp, other))
    act_in[pl.ds(x, 1)] = act_out[pl.ds(x, 1)]

    for n in (0, 10, 11):
        loads[n].wait()
    settle(act_in.at[pl.ds(0, 3)], small_recv.at[2])
    channels = jnp.concatenate([act_in[m] for m in range(4)], axis=1)
    total = jnp.zeros((48, 1), F32)
    for c in range(CHUNKS):
        cols = pl.ds(WIDE * c, WIDE)
        v = deep_alpha * residual[:, cols].astype(F32) + dot(channels, project[:, cols])
        middle[:, cols] = v
        total = total + jnp.sum(v, axis=1, keepdims=True)
    mean = total / (CHUNKS * WIDE)
    total = jnp.zeros((48, 1), F32)
    for c in range(CHUNKS):
        center = middle[:, pl.ds(WIDE * c, WIDE)] - mean
        total = total + jnp.sum(center * center, axis=1, keepdims=True)
    factor = lax.rsqrt(total / (CHUNKS * WIDE) + norm_epsilon)
    for c in range(CHUNKS):
        cols = pl.ds(WIDE * c, WIDE)
        v = (middle[:, cols] - mean) * factor * norm_gain[:, cols]
        middle[:, cols] = v
        rows[pl.ds(0, 48), cols] = v.astype(BF16)
        out1[:, :, cols] = dot(taken[...], rows[:, cols]).astype(BF16).reshape(8, 16, WIDE)
        for k in FAR:
            other, device = yc_peer(k)
            send(out1.at[other, :, cols], in1.at[yc, :, cols], yc_send.at[0], yc_recv.at[0, c], device)
        in1[pl.ds(yc, 1), :, cols] = out1[pl.ds(yc, 1), :, cols]

    def side(h):
        return pl.ds(HALF * h, HALF)

    def start_z(i, h, cols):
        to = LANDS[i]
        send(
            out2.at[i, :, cols], xin.at[0, to, :, cols], z_send.at[0], z_recv.at[to, h],
            z_peer(ORDER[i])[1],
        )

    def spread(i, h, cols):
        block = xin.at[0, i, :, cols]
        rest = o_recv.at[i // 4]
        send(block, xin.at[1, i, :, cols], x_send.at[0], rest if h else x_recv.at[0, i], (sp, right))
        send(block, xin.at[2, i, :, cols], x_send.at[1], x_recv.at[1, i] if h else rest, (sp, left))

    def pass_on(i, h):
        block = xin.at[1 + h, i, :, side(h)]
        settle(block, x_recv.at[h, i])
        send(block, xin.at[3, i, :, side(h)], x_send.at[2 + h], o_recv.at[i // 4], (sp, (right, left)[h]))

    for c in range(CHUNKS):
        cols = pl.ds(WIDE * c, WIDE)
        settle(in1.at[pl.ds(0, 7), :, cols], yc_recv.at[0, c])
        moved = dot(swap[...], in1[:, :, cols].reshape(128, WIDE)).astype(BF16)
        out2[:, :, cols] = moved.reshape(8, 16, WIDE)
        xin[0, 0, :, cols] = moved[0:16, :]
        for i in range(1, 4):
            start_z(i, c // 2, cols)
        spread(0, c // 2, cols)
    for i in range(4, 5):
        for h in range(2):
            start_z(i, h, side(h))

    def multiply(g):
        settle(xin.at[pl.ds(2, 2), pl.ds(4 * g, 4)], o_recv.at[g])
        block = xin[:, pl.ds(4 * g, 4)].reshape(256, 2048)
        gate = dot(block, w_gate[...])
        linear = dot(block, w_linear[...])
        hidden[g] = (gate / (1.0 + jnp.exp(-gate)) * linear).astype(BF16)

    low, high = pl.ds(0, 2), pl.ds(2, 2)

    def start_sums(g, c):
        cols = pl.ds(WIDE * c, WIDE)
        part = dot(hidden[g], w_down[:, cols]).reshape(4, 4, 16, WIDE)
        opp_out[g, :, :, cols] = part[3].astype(BF16)
        send(opp_out.at[g, low, :, cols], fwd.at[0, g, :, :, cols], rs_send.at[0], rs_recv.at[0, g, c], (sp, right))
        send(opp_out.at[g, high, :, cols], fwd.at[1, g, :, :, cols], rs_send.at[1], rs_recv.at[2, g, c], (sp, left))
        right_out[g, high, :, cols] = part[2, 2:4].astype(BF16)
        keep_r[g, :, :, cols] = part[2, 0:2]
        send(right_out.at[g, high, :, cols], sums.at[0, g, high, :, cols], rs_send.at[2], rs_recv.at[1, g, c], (sp, right))
        left_out[g, low, :, cols] = part[1, 0:2].astype(BF16)
        keep_l[g, :, :, cols] = part[1, 2:4]
        send(left_out.at[g, low, :, cols], sums.at[1, g, low, :, cols], rs_send.at[3], rs_recv.at[1, g, c], (sp, left))
        keep_o[g, :, :, cols] = part[0]

    def add_on(g, c):
        cols = pl.ds(WIDE * c, WIDE)
        settle(fwd.at[0, g, :, :, cols], rs_recv.at[0, g, c])
        right_out[g, low, :, cols] = (keep_r[g, :, :, cols] + fwd[0, g, :, :, cols].astype(F32)).astype(BF16)
        send(right_out.at[g, low, :, cols], sums.at[0, g, low, :, cols], rs_send.at[2], rs_recv.at[1, g, c], (sp, right))
        settle(fwd.at[1, g, :, :, cols], rs_recv.at[2, g, c])
        left_out[g, high, :, cols] = (keep_l[g, :, :, cols] + fwd[1, g, :, :, cols].astype(F32)).astype(BF16)
        send(left_out.at[g, high, :, cols], sums.at[1, g, high, :, cols], rs_send.at[3], rs_recv.at[1, g, c], (sp, left))

    def finish_sums(g, c):
        cols = pl.ds(WIDE * c, WIDE)
        settle(sums.at[:, g, :, :, cols], rs_recv.at[1, g, c])
        part = keep_o[g, :, :, cols] + sums[0, g, :, :, cols].astype(F32) + sums[1, g, :, :, cols].astype(F32)
        ans[pl.ds(4 * g, 4), :, cols] = part.astype(BF16)
        for i in range(4 * g, 4 * g + 4):
            if i == 0:
                b2in[0, :, cols] = ans[0, :, cols]
                continue
            send(ans.at[i, :, cols], b2in.at[LANDS[i], :, cols], z_send.at[1], z_back.at[c], z_peer(ORDER[i])[1])

    def go_home(c):
        cols = pl.ds(WIDE * c, WIDE)
        settle(b2in.at[pl.ds(0, 7), :, cols], z_back.at[c])
        moved = dot(swap[...], b2in[:, :, cols].reshape(128, WIDE)).astype(BF16)
        b2out[:, :, cols] = moved.reshape(8, 16, WIDE)
        for k in FAR:
            other, device = yc_peer(k)
            send(b2out.at[other, :, cols], b1in.at[yc, :, cols], yc_send.at[1], yc_recv.at[1, c], device)
        b1in[pl.ds(yc, 1), :, cols] = b2out[pl.ds(yc, 1), :, cols]

    for i in range(1, 8):
        for h in range(2):
            settle(xin.at[0, i, :, side(h)], z_recv.at[i, h])
            spread(i, h, side(h))
            if i == 1:
                pass_on(0, h)
        for later in {1: (5,), 2: (6,), 3: (7,)}.get(i, ()):
            for h in range(2):
                start_z(later, h, side(h))
        passed = {2: 1, 3: 2, 5: 3, 6: 4, 7: 5}.get(i)
        if passed is not None:
            pass_on(passed, 0)
            pass_on(passed, 1)
        if i == 1:
            for n in (15, 16, 17):
                loads[n].wait()
    multiply(0)
    pass_on(6, 0)
    pass_on(6, 1)
    pass_on(7, 0)
    pass_on(7, 1)
    start_sums(0, 0)
    start_sums(0, 1)
    multiply(1)
    start_sums(1, 0)
    start_sums(1, 1)
    add_on(0, 0)
    add_on(0, 1)
    start_sums(1, 2)
    add_on(1, 0)
    start_sums(1, 3)
    add_on(1, 1)
    start_sums(0, 2)
    start_sums(0, 3)
    finish_sums(0, 0)
    add_on(1, 2)
    finish_sums(0, 1)
    finish_sums(1, 0)
    add_on(1, 3)
    finish_sums(1, 1)
    add_on(0, 2)
    finish_sums(1, 2)
    add_on(0, 3)
    finish_sums(1, 3)
    finish_sums(0, 2)
    finish_sums(0, 3)
    for c in range(CHUNKS):
        go_home(c)

    total = jnp.zeros((48, 1), F32)
    for c in range(CHUNKS):
        cols = pl.ds(WIDE * c, WIDE)
        settle(b1in.at[pl.ds(0, 7), :, cols], yc_recv.at[1, c])
        back = b1in[:, :, cols].reshape(128, WIDE)
        routed = dot(combine[0, pl.ds(0, 48), :], back) + dot(combine[1, pl.ds(0, 48), :], back)
        v = deep_alpha * middle[:, cols] + routed
        middle[:, cols] = v
        total = total + jnp.sum(v, axis=1, keepdims=True)
    mean = total / (CHUNKS * WIDE)
    total = jnp.zeros((48, 1), F32)
    for c in range(CHUNKS):
        center = middle[:, pl.ds(WIDE * c, WIDE)] - mean
        total = total + jnp.sum(center * center, axis=1, keepdims=True)
    factor = lax.rsqrt(total / (CHUNKS * WIDE) + norm_epsilon)
    for c in range(CHUNKS):
        cols = pl.ds(WIDE * c, WIDE)
        out[:, cols] = (middle[:, cols] - mean) * factor

    settle(recv1.at[pl.ds(0, 7)], small_send.at[0])
    settle(recv2.at[pl.ds(0, 7), 0], small_send.at[1])
    settle(keep1.at[pl.ds(0, 7)], small_send.at[3])
    settle(keep2.at[pl.ds(0, 7)], small_send.at[4])
    settle(act_in.at[pl.ds(0, 3)], small_send.at[2])
    for index in range(2):
        settle(out1.at[pl.ds(0, 7)], yc_send.at[index])
        settle(out2.at[pl.ds(0, 7)], z_send.at[index])
        settle(xin.at[0], x_send.at[index])
        settle(xin.at[0, pl.ds(0, 4)], x_send.at[2 + index])
        settle(fwd.at[0], rs_send.at[index])
        settle(sums.at[0], rs_send.at[2 + index])


def on_device(
    residual, mixer_input, log_gate, decay_rate, turn_rate, drive_real, drive_imaginary, read_real,
    read_imaginary, skip_gain, project_weight, norm_gain, final_gain, routes, group_weight,
    expert_weight, gate_weight, linear_weight, down_weight,
):
    dma = pltpu.SemaphoreType.DMA
    slab = pltpu.VMEM((8, 16, 2048), BF16)
    groups = pltpu.VMEM((2, 4, 16, 2048), BF16)
    normed = pl.pallas_call(
        kernel,
        out_shape=jax.ShapeDtypeStruct((48, 2048), F32),
        in_specs=[pl.BlockSpec(memory_space=pl.ANY)] * len(INPUTS),
        out_specs=pl.BlockSpec(memory_space=pltpu.VMEM),
        scratch_shapes=[pltpu.VMEM(shape, dtype) for shape, dtype in INPUTS]
        + [
            pltpu.VMEM((4, 192, 128), F32),
            pltpu.VMEM((4, 4, 192, 128), F32),
            pltpu.VMEM((2, 8, 128), F32),
            pltpu.VMEM((8, 2, 8, 128), F32),
            pltpu.VMEM((2, 8, 128), F32),
            pltpu.VMEM((8, 2, 8, 128), F32),
            pltpu.VMEM((1, 1, 512), F32),
            pltpu.VMEM((8, 1, 512), F32),
            pltpu.VMEM((1, 1, 512), F32),
            pltpu.VMEM((8, 1, 512), F32),
            pltpu.VMEM((4, 48, 128), BF16),
            pltpu.VMEM((4, 48, 128), BF16),
            pltpu.VMEM((48, 2048), F32),
            pltpu.VMEM((128, 2048), BF16),
            pltpu.VMEM((4, 2, 256, 256), BF16),
            pltpu.VMEM((128, 128), BF16),
            pltpu.VMEM((2, 128, 128), BF16),
            pltpu.VMEM((128, 128), BF16),
            slab, slab, slab,
            pltpu.VMEM((4, 8, 16, 2048), BF16),
            pltpu.VMEM((2, 256, 256), BF16),
            groups,
            pltpu.VMEM((2, 2, 2, 16, 2048), BF16),
            groups, groups,
            pltpu.VMEM((2, 2, 4, 16, 2048), BF16),
            pltpu.VMEM((2, 2, 16, 2048), F32),
            pltpu.VMEM((2, 2, 16, 2048), F32),
            pltpu.VMEM((2, 4, 16, 2048), F32),
            slab, slab, slab, slab,
            dma((len(INPUTS),)), dma((5,)), dma((5,)),
            dma((2,)), dma((2, CHUNKS)), dma((2,)), dma((8, 2)), dma((CHUNKS,)),
            dma((4,)), dma((2, 8)), dma((2,)),
            dma((4,)), dma((3, 2, CHUNKS)),
        ],
        compiler_params=pltpu.CompilerParams(
            collective_id=0, has_side_effects=True, vmem_limit_bytes=40 * 1024 * 1024
        ),
        name="layer",
    )(*(pltpu.with_memory_space_constraint(v, pltpu.HBM) for v in (
        residual, mixer_input, log_gate.T, decay_rate, turn_rate,
        drive_real.reshape(256, 64), drive_imaginary.reshape(256, 64),
        read_real.reshape(256, 64), read_imaginary.reshape(256, 64),
        skip_gain.reshape(1, 128), project_weight, norm_gain.reshape(1, 2048),
        routes.T, group_weight.reshape(1, 192), expert_weight.T,
        gate_weight[0], linear_weight[0], down_weight[0],
    )))
    return (normed * final_gain).astype(BF16)


def solution(mesh):
    placed = (
        P(("sp", "tp"), None),
        P("sp", "tp"),
        P("sp", "tp"),
        P(None, "tp", None),
        P(None, "tp", None),
        P(None, "tp", None, None),
        P(None, "tp", None, None),
        P(None, "tp", None, None),
        P(None, "tp", None, None),
        P("tp"),
        P(),
        P(),
        P(),
        P("sp", None),
        P("sp"),
        P("sp", None),
        P("sp", None, "tp"),
        P("sp", None, "tp"),
        P("sp", "tp", None),
    )
    return jax.shard_map(
        on_device, mesh=mesh, in_specs=placed, out_specs=P(("sp", "tp"), None), check_vma=False
    )
```
